32 devices in a mesh: sp: 8 (over z, y), tp: 4 (over x, core).
Axes of the slice: x: 2, y: 2, z: 4, core: 2. Of those that a mesh axis runs over, the one named last changes fastest.
Arguments:
- tokens: bfloat16 [4096, 2048], P(('sp', 'tp')), may hold values from -6 to 6
- norm_gain: float32 [2048], replicated, may hold values from 0.25 to 5
- w_query_one: bfloat16 [2048, 512], P(None, 'tp'), may hold values from -0.21875 to 0.21875
- w_query_two: bfloat16 [2048, 512], P(None, 'tp'), may hold values from -0.21875 to 0.21875
- w_key_one: bfloat16 [2048, 512], P(None, 'tp'), may hold values from -0.125 to 0.125
- w_key_two: bfloat16 [2048, 512], P(None, 'tp'), may hold values from -0.125 to 0.125
- w_value: bfloat16 [2048, 1024], P(None, 'tp'), may hold values from -0.125 to 0.125
- mix_lambda: float32 [8], P('tp'), may hold values from 0.3 to 0.8
- head_gain: float32 [128], replicated, may hold values from 0.1 to 1.9
- w_ret_query: bfloat16 [2048, 512], P(None, 'tp'), may hold values from -0.125 to 0.125
- w_ret_key: bfloat16 [2048, 512], P(None, 'tp'), may hold values from -0.125 to 0.125
- w_ret_value: bfloat16 [2048, 1024], P(None, 'tp'), may hold values from -0.125 to 0.125
- retain_log: float32 [8, 4096], P('tp', 'sp'), may hold values from -1 to 0
- init_state: float32 [8, 64, 128], P('tp'), may hold values from -144 to 144
- w_out_diff: bfloat16 [1024, 2048], P('tp'), may hold values from -0.125 to 0.125
- w_out_ret: bfloat16 [1024, 2048], P('tp'), may hold values from -0.125 to 0.125
Outputs:
- mixed: bfloat16 [4096, 2048], P(('sp', 'tp'))
The draws below stay inside these ranges and needn't reach their ends.
All inputs are finite; a program needn't handle non-finite values.
Results may differ from the reference program's by a relative error of at most 0.015.
The reference program's roundings to bfloat16 on the way count: a program that leaves them out, or rounds other values in their place, can miss the bound.
Values may be sent and summed in bfloat16 or wider, within the bound.
A program may use at most 128 MiB of HBM per device.

```python
import math
import jax
import jax.numpy as jnp
from jax import lax

D = 2048
HEADS_DIFF = 8
HEADS_RET = 8
HEAD = 64
VAL = 128
BLOCK = 256
TOK_DEV = 512
TOKENS = 4096


def draw_retain_log(key, part):
    keys = jax.random.split(jax.random.fold_in(key, 11), 7)
    slow = jax.random.bernoulli(keys[0], 0.5, (HEADS_RET,))
    slow_rate = jax.random.uniform(keys[1], (HEADS_RET,), minval=0.1, maxval=0.3) / TOKENS
    fast_rate = jnp.exp(jax.random.uniform(keys[2], (HEADS_RET,), minval=math.log(1.0 / 100.0), maxval=math.log(1.0 / 30.0)))
    fading_speed = jnp.where(slow, slow_rate, fast_rate)
    pace = jnp.exp(jax.random.uniform(keys[3], (TOKENS // TOK_DEV,), minval=-0.7, maxval=0.7))
    fading_speeds_list = jnp.repeat(pace, TOK_DEV)
    sampled_displacement = jnp.exp(jax.random.uniform(keys[4], (HEADS_RET, TOKENS), minval=-0.5, maxval=0.5))
    sequence_indices = jax.random.randint(keys[5], (HEADS_RET, 3), 0, TOKENS)
    stack_level = jnp.log(jax.random.uniform(keys[6], (HEADS_RET, 3), minval=0.5, maxval=0.8))
    sequence_index = jnp.arange(TOKENS, dtype=jnp.int32)
    cluster_sets = jnp.sum(jnp.where(sequence_index[None, None, :] == sequence_indices[:, :, None], stack_level[:, :, None], 0.0), axis=1)
    return (-fading_speed[:, None] * fading_speeds_list[None, :] * sampled_displacement + cluster_sets).astype(jnp.float32)


def draw_norm_gain(key, part):
    inner = jax.random.fold_in(key, 23)
    gains = 1.0 + 0.18 * jax.random.truncated_normal(inner, -4.0, 4.0, (D,))
    return gains.astype(jnp.float32)


def block_levels(stream_key, extent, pieces, low, largest):
    loudness, own = 1.0, jax.random.fold_in(stream_key, 6)
    for axis_at, parts in pieces:
        steps = jnp.exp(jax.random.uniform(jax.random.fold_in(own, axis_at), (parts,), jnp.float32, low / len(pieces), largest / len(pieces)))
        loudness = loudness * jnp.repeat(steps, extent[axis_at] // parts).reshape([-1 if axis == axis_at else 1 for axis in range(len(extent))])
    return loudness


def normal_values(own_key, dims, width, most, cuts=(), kind=jnp.bfloat16):
    gain = block_levels(own_key, dims, cuts, -0.22, 0.18) if cuts else 1.0
    entries = jax.random.normal(own_key, dims, jnp.float32) * width * gain
    return jnp.minimum(jnp.maximum(entries, -most), most).astype(kind)


def setup_inputs(seed: int = 0) -> dict:
    seeds = jax.random.split(jax.random.key(seed), 17)
    return {
        "tokens": normal_values(seeds[0], (TOKENS, D), 1.0, 6.0, ((0, 32),)),
        "norm_gain": draw_norm_gain(jax.random.fold_in(seeds[16], 71), 0),
        "w_query_one": normal_values(seeds[2], (D, HEADS_DIFF * HEAD), (D // 3) ** -0.5, 0.21875, ((1, 4),)),
        "w_query_two": normal_values(seeds[3], (D, HEADS_DIFF * HEAD), (D // 3) ** -0.5, 0.21875, ((1, 4),)),
        "w_key_one": normal_values(seeds[4], (D, HEADS_DIFF * HEAD), D ** -0.5, 0.125, ((1, 4),)),
        "w_key_two": normal_values(seeds[5], (D, HEADS_DIFF * HEAD), D ** -0.5, 0.125, ((1, 4),)),
        "w_value": normal_values(seeds[6], (D, HEADS_DIFF * VAL), D ** -0.5, 0.125, ((1, 4),)),
        "mix_lambda": jnp.clip(0.3 + 0.5 * jax.random.uniform(seeds[7], (HEADS_DIFF,), jnp.float32) ** block_levels(seeds[7], (HEADS_DIFF,), ((0, 4),), -0.2, 0.2), 0.3, 0.8),
        "head_gain": jnp.clip(1.0 + 0.18 * jax.random.normal(seeds[8], (VAL,), jnp.float32), 0.1, 1.9),
        "w_ret_query": normal_values(seeds[9], (D, HEADS_RET * HEAD), D ** -0.5, 0.125, ((1, 4),)),
        "w_ret_key": normal_values(seeds[10], (D, HEADS_RET * HEAD), D ** -0.5, 0.125, ((1, 4),)),
        "w_ret_value": normal_values(seeds[11], (D, HEADS_RET * VAL), D ** -0.5, 0.125, ((1, 4),)),
        "retain_log": draw_retain_log(jax.random.fold_in(seeds[16], 71), 0),
        "init_state": normal_values(seeds[13], (HEADS_RET, HEAD, VAL), 24.0, 144.0, ((0, 4),), jnp.float32),
        "w_out_diff": normal_values(seeds[14], (HEADS_DIFF * VAL, D), ((HEADS_DIFF + HEADS_RET) * VAL) ** -0.5, 0.125, ((0, 4),)),
        "w_out_ret": normal_values(seeds[15], (HEADS_RET * VAL, D), ((HEADS_DIFF + HEADS_RET) * VAL) ** -0.5, 0.125, ((0, 4),)),
    }


NORM_EPS = 1e-06
HEAD_EPS = 1e-05
DIFF_SCALE = 0.8
HIGHEST = lax.Precision.HIGHEST

def head_norm(values):
    return values * lax.rsqrt(lax.optimization_barrier(jnp.mean(values * values, axis=-1, keepdims=True)) + HEAD_EPS)

def diff_head(query_one, query_two, key_one, key_two, values, weight_two):
    total_rows = query_one.shape[0]
    block_rows = math.gcd(total_rows, 512)
    key_pos = jnp.arange(total_rows, dtype=jnp.int32)

    def one_block(number):
        begin_at = (number * block_rows).astype(jnp.int32)
        allowed = (begin_at + jnp.arange(block_rows, dtype=jnp.int32))[:, None] >= key_pos[None, :]

        def soft_map(query, keys):
            portion = lax.dynamic_slice_in_dim(query, begin_at, block_rows, 0)
            scores = jnp.dot(portion, keys.T, preferred_element_type=jnp.float32) * HEAD ** (-0.5)
            scores = jnp.where(allowed, scores, -jnp.inf)
            shifted = jnp.exp(scores - lax.optimization_barrier(jnp.max(scores, axis=-1, keepdims=True)))
            weighted = jnp.dot(shifted.astype(jnp.bfloat16), values, preferred_element_type=jnp.float32)
            return weighted / lax.optimization_barrier(jnp.sum(shifted, axis=-1, keepdims=True))
        return soft_map(query_one, key_one) - weight_two * soft_map(query_two, key_two)
    blocks = lax.map(one_block, jnp.arange(total_rows // block_rows, dtype=jnp.int32))
    return blocks.reshape(total_rows, VAL)

def retention(ret_query, ret_key, ret_value, retain_log, init_state):
    nblocks = TOKENS // BLOCK

    def split_blocks(data, size):
        return data.reshape(nblocks, BLOCK, HEADS_RET, size).transpose(0, 2, 1, 3)
    block_query = split_blocks(ret_query, HEAD)
    block_key = split_blocks(ret_key, HEAD)
    block_value = split_blocks(ret_value, VAL)
    log_blocks = retain_log.reshape(HEADS_RET, nblocks, BLOCK).transpose(1, 0, 2)
    sequence_index = jnp.arange(BLOCK, dtype=jnp.int32)
    causal = sequence_index[:, None] >= sequence_index[None, :]

    def ret_step(memory, inputs):
        query, keys, values, logs = inputs
        query_f = query.astype(jnp.float32)
        keys_f = keys.astype(jnp.float32)
        values_f = values.astype(jnp.float32)
        cumulative = jnp.cumsum(logs, axis=-1)
        gap_log = jnp.where(causal[None], cumulative[:, :, None] - cumulative[:, None, :], -jnp.inf)
        raw = jnp.einsum('hqd,hkd->hqk', query_f, keys_f, precision=HIGHEST)
        decayed = (raw * HEAD ** (-0.5) * jnp.exp(gap_log)).astype(jnp.bfloat16).astype(jnp.float32)
        result = jnp.einsum('hqk,hke->hqe', decayed, values_f, precision=HIGHEST)
        result = result + jnp.einsum('hqd,hde->hqe', query_f * jnp.exp(cumulative)[:, :, None], memory, precision=HIGHEST)
        last_log = cumulative[:, -1:]
        key_scaled = (keys_f * HEAD ** (-0.5) * jnp.exp(last_log - cumulative)[:, :, None]).astype(jnp.bfloat16).astype(jnp.float32)
        memory = jnp.exp(last_log)[:, :, None] * memory + jnp.einsum('hkd,hke->hde', key_scaled, values_f, precision=HIGHEST)
        return (memory, result)
    final_state, outputs = lax.scan(ret_step, init_state, (block_query, block_key, block_value, log_blocks))
    outputs = outputs.transpose(0, 2, 1, 3).reshape(TOKENS, HEADS_RET, VAL)
    return head_norm(outputs).reshape(TOKENS, HEADS_RET * VAL).astype(jnp.bfloat16)

def reference(tokens, norm_gain, w_query_one, w_query_two, w_key_one, w_key_two, w_value, mix_lambda, head_gain, w_ret_query, w_ret_key, w_ret_value, retain_log, init_state, w_out_diff, w_out_ret):
    floats = tokens.astype(jnp.float32)
    normed = (floats * lax.rsqrt(lax.optimization_barrier(jnp.mean(floats * floats, axis=-1, keepdims=True)) + NORM_EPS) * norm_gain).astype(jnp.bfloat16)

    def project(weight):
        return jnp.dot(normed, weight, preferred_element_type=jnp.float32).astype(jnp.bfloat16)
    query_one = project(w_query_one).reshape(TOKENS, HEADS_DIFF, HEAD)
    query_two = project(w_query_two).reshape(TOKENS, HEADS_DIFF, HEAD)
    key_one = project(w_key_one).reshape(TOKENS, HEADS_DIFF, HEAD)
    key_two = project(w_key_two).reshape(TOKENS, HEADS_DIFF, HEAD)
    values = project(w_value).reshape(TOKENS, HEADS_DIFF, VAL)
    head_outs = []
    for number in range(HEADS_DIFF):
        head_outs.append(diff_head(query_one[:, number], query_two[:, number], key_one[:, number], key_two[:, number], values[:, number], mix_lambda[number]))
    mixed_heads = jnp.stack(head_outs, axis=1)
    diff_out = (head_norm(mixed_heads) * head_gain * DIFF_SCALE).reshape(TOKENS, HEADS_DIFF * VAL).astype(jnp.bfloat16)
    ret_out = retention(project(w_ret_query), project(w_ret_key), project(w_ret_value), retain_log, init_state)
    total = jnp.dot(diff_out, w_out_diff, preferred_element_type=jnp.float32) + jnp.dot(ret_out, w_out_ret, preferred_element_type=jnp.float32)
    return total.astype(jnp.bfloat16)
```

```python
import functools

import jax
import jax.numpy as jnp
from jax import lax
from jax.experimental import pallas as pl
from jax.experimental.pallas import tpu as pltpu
from jax.sharding import PartitionSpec as P

BLOCK = 256
SQUARE = 4
NORM_EPS = 1e-06
HEAD_EPS = 1e-05
DIFF_SCALE = 0.8
HIGHEST = lax.Precision.HIGHEST
MESH = pl.DeviceIdType.MESH
F32 = jnp.float32
BF16 = jnp.bfloat16
VMEM_LIMIT = 60 * 1024 * 1024


def remote(src, dst, send, recv, where):
    return pltpu.make_async_remote_copy(
        src_ref=src, dst_ref=dst, send_sem=send, recv_sem=recv,
        device_id=where, device_id_type=MESH,
    )


def head_norm(values):
    return values * lax.rsqrt(jnp.mean(values * values, axis=-1, keepdims=True) + HEAD_EPS)


def nn(a, b, **kw):
    return lax.dot_general(a, b, (((1,), (0,)), ((), ())), preferred_element_type=F32, **kw)


def nt(a, b):
    return lax.dot_general(a, b, (((1,), (1,)), ((), ())), preferred_element_type=F32)


def tn(a, b):
    return lax.dot_general(a, b, (((0,), (0,)), ((), ())), preferred_element_type=F32)


def layer_kernel(nsp, ntp, widths, heads, rheads, lam_ref, tokens_ref, ngain_ref, gain_ref, log_ref,
                 init_ref, *refs):
    nw = len(widths)
    w_refs = refs[:nw]
    wd_ref, wr_ref, out_ref = refs[nw : nw + 3]
    (gat, wbuf, wobuf, sndq, sndkv, kvb, qraw, qs, lamv, peak, den, acc, dsend, dret, sts, rbuf, rmid,
     upd, mixr, mine, sent, from_pair, from_chip, wsem, lsem, pair_send, cross_send, grecv, sq_sem,
     skv_sem, inter_sem, fwd_sem, rq_sem, rkv_sem, ds_sem, rd_sem, sem_zs, sem_ys, sem_rs,
     mpair_send, mpair_recv, mchip_send, mchip_recv) = refs[nw + 3 :]
    me = lax.axis_index("sp")
    b = lax.rem(me, 2)
    p = me // 2
    npair = nsp // 2
    ngroup = nsp // SQUARE
    g = me // SQUARE
    s = lax.rem(me, SQUARE)
    up = {"sp": lax.rem(me + 2, nsp)}
    side = {"sp": me + 1 - 2 * b}
    tme = lax.axis_index("tp")
    core = lax.rem(tme, 2)
    chip = tme // 2
    nchip = ntp // 2
    tpair = tme + 1 - 2 * core
    pair = {"tp": tpair}
    own_rows = tokens_ref.shape[0]
    rows = own_rows * ntp
    chunk = rows // nchip
    kw = widths[2]
    hd = kw // heads
    val = gain_ref.shape[1]
    first_up = p < npair - 1

    held = (core, SQUARE - 1 - core)
    others = (1 - core, 2 + core)
    land = lax.rem((s + 1) // 2, 2)
    head_core = s // 2
    head_no = lax.rem(s, 2)
    base = SQUARE * g

    barrier = pltpu.get_barrier_semaphore()

    def greet(where):
        pl.semaphore_signal(barrier, inc=1, device_id=where, device_id_type=MESH)

    for k in range(1, ntp):
        greet({"tp": lax.rem(tme + k, ntp)})
    for k in range(1, SQUARE):
        for n in range(ntp):
            greet({"sp": base + lax.rem(s + k, SQUARE), "tp": n})
    for dg in range(1, ngroup):

        @pl.when(g + dg < ngroup)
        def _():
            for h in range(2):
                greet({"sp": base + SQUARE * dg + 2 * core + h, "tp": chip * 2 + land})

        @pl.when(g >= dg)
        def _():
            for t in range(2):
                greet({"sp": base - SQUARE * dg + held[t], "tp": chip * 2 + head_core})

    above = (s >= 2) & (g < ngroup - 1)
    below = (s < 2) & (g > 0)

    @pl.when(above)
    def _():
        greet(up)

    @pl.when(below)
    def _():
        greet({"sp": me - 2})

    order = (0, 1, 2, 3, 4, 5, 6, 7)
    starts = [sum(widths[:n]) for n in range(nw)]
    loads = {}
    for n in order:
        at = starts[n]
        loads[n] = pltpu.make_async_copy(w_refs[n], wbuf.at[:, at : at + widths[n]], wsem.at[n])
        loads[n].start()
    depth = wd_ref.shape[0]
    out_loads = [
        pltpu.make_async_copy(wd_ref, wobuf.at[:depth], wsem.at[nw]),
        pltpu.make_async_copy(wr_ref, wobuf.at[depth:], wsem.at[nw + 1]),
    ]
    for load in out_loads:
        load.start()
    floats = tokens_ref[...].astype(F32)
    gat[tme] = (
        floats * lax.rsqrt(jnp.mean(floats * floats, axis=-1, keepdims=True) + NORM_EPS) * ngain_ref[...]
    ).astype(BF16)
    for h in range(heads):
        lamv[core, 8 * h : 8 * h + 8, :] = jnp.full((8, 128), lam_ref[h], F32)
    pl.semaphore_wait(
        barrier,
        (ntp - 1) + (SQUARE - 1) * ntp + 2 * (ngroup - 1)
        + above.astype(jnp.int32) + below.astype(jnp.int32),
    )
    copies = []

    def begin(copy):
        copies.append(copy)
        copy.start()

    def slab(which, half):
        return gat.at[which, pl.ds(half * (own_rows // 2), own_rows // 2)]

    for d in range(1, nchip):
        there = {"tp": lax.rem(chip + d, nchip) * 2 + core}
        for half in range(2):
            begin(remote(slab(tme, half), slab(tme, half), cross_send.at[d, half],
                         grecv.at[tme, half], there))

    def to_pair(which, half):
        begin(remote(slab(which, half), slab(which, half), pair_send.at[which // 2, half],
                     grecv.at[which, half], pair))

    def landed(which, half):
        remote(slab(which, half), slab(which, half), pair_send.at[which // 2, half],
               grecv.at[which, half], pair).wait_recv()

    def lam_copy(who):
        return remote(lamv.at[who], lamv.at[who], lsem.at[0], lsem.at[1], pair)

    def part(d):
        return lax.rem(chip + nchip - d, nchip)

    def keys_at(d):
        return pl.ds(pl.multiple_of(part(d) * chunk, chunk), chunk)

    def q_copy(h, d):
        where = {"sp": base + 2 * core + h, "tp": chip * 2 + land}
        return remote(sndq.at[h, part(d)], qraw.at[s // 2, part(d)], sq_sem.at[h, d],
                      rq_sem.at[s // 2, d], where)

    def kv_copy(h, d, dg):
        where = {"sp": base + SQUARE * dg + 2 * core + h, "tp": chip * 2 + land}
        sem = skv_sem.at[h, d] if dg == 0 else inter_sem.at[dg - 1, h, d]
        return remote(sndkv.at[h, part(d)], kvb.at[me, part(d)], sem, rkv_sem.at[me, d], where)

    def q_local(h, d):
        return pltpu.make_async_copy(sndq.at[h, part(d)], qraw.at[s // 2, part(d)], rq_sem.at[s // 2, d])

    def kv_local(h, d):
        return pltpu.make_async_copy(sndkv.at[h, part(d)], kvb.at[me, part(d)], rkv_sem.at[me, d])

    def stays(h):
        return (2 * core + h == s) & (land == core)

    def fwd(span, t, dg, d):
        piece = kvb.at[span, part(d)]
        return remote(piece, piece, fwd_sem.at[dg, t, d], rkv_sem.at[span, d], pair)

    lane = lax.broadcasted_iota(jnp.int32, (chunk, 128), 1)

    def project(d):
        both = gat[pl.ds(part(d) * 2, 2)].reshape(chunk, gat.shape[2])

        def product(lo, hi):
            if d == 0:
                for n in range(lo, hi):
                    loads[n].wait()
            span = sum(widths[lo:hi])
            return nn(both, wbuf[:, starts[lo] : starts[lo] + span]).astype(BF16).astype(F32)

        def by_head(pairs):
            one, two = pairs[:, :kw], pairs[:, kw:]
            return (jnp.where(lane < hd, one, pltpu.roll(two, hd, 1)),
                    jnp.where(lane < hd, pltpu.roll(one, kw - hd, 1), two))

        queries = by_head(product(0, 2) * hd ** (-0.5))
        for h in range(heads):
            sndq[h, part(d)] = queries[h].astype(BF16)
        keys = by_head(product(2, 4))
        values = product(4, 5)
        for h in range(heads):
            sndkv[h, part(d), :chunk] = keys[h].astype(BF16)
            turned = values[:, h * val : (h + 1) * val].T.astype(BF16)
            for c in range(chunk // 128):
                at = chunk + c * val
                sndkv[h, part(d), at : at + val] = turned[:, c * 128 : (c + 1) * 128]
        for h in range(heads):

            @pl.when(stays(h))
            def _():
                q_local(h, d).start()
                kv_local(h, d).start()

            @pl.when(jnp.logical_not(stays(h)))
            def _():
                q_copy(h, d).start()
                kv_copy(h, d, 0).start()

        for dg in range(1, ngroup):

            @pl.when(g + dg < ngroup)
            def _():
                for h in range(heads):
                    kv_copy(h, d, dg).start()

    def project_ret(d):
        both = gat[pl.ds(part(d) * 2, 2)].reshape(chunk, gat.shape[2])
        if d == 0:
            for n in range(5, 8):
                loads[n].wait()
        span = sum(widths[5:8])
        for c in range(0, span, 256):
            rbuf[keys_at(d), c : c + 256] = nn(
                both, wbuf[:, starts[5] + c : starts[5] + c + 256]).astype(BF16)

    def st_copy(i, j, sem, where):
        return remote(sts.at[j], sts.at[j], sem.at[i], sem_rs.at[j], where)

    def relay(i):
        jz = 2 * (p - i) + b

        @pl.when(i <= p)
        def _():
            st_copy(i, jz, sem_zs, up).wait_recv()

            @pl.when(first_up)
            def _():
                st_copy(i, jz, sem_zs, up).start()

            st_copy(i, jz, sem_ys, side).start()

    for half in range(2):
        to_pair(tme, half)
    begin(lam_copy(core))
    peak[...] = jnp.full(peak.shape, -jnp.inf, F32)
    den[...] = jnp.zeros(den.shape, F32)
    acc[...] = jnp.zeros(acc.shape, F32)
    for half in range(2):
        landed(tpair, half)
    project(0)
    project_ret(0)

    def take(span, t, d, local):
        if local:
            here = (held[t] == s) & (head_core == core)

            @pl.when(here)
            def _():
                q_local(0, d).wait()
                kv_local(0, d).wait()

            @pl.when(jnp.logical_not(here))
            def _():
                remote(qraw.at[t, part(d)], qraw.at[t, part(d)], sq_sem.at[0, d],
                       rq_sem.at[t, d], pair).wait_recv()
                remote(kvb.at[span, part(d)], kvb.at[span, part(d)], skv_sem.at[0, d],
                       rkv_sem.at[span, d], pair).wait_recv()
        else:
            remote(kvb.at[span, part(d)], kvb.at[span, part(d)], skv_sem.at[0, d],
                   rkv_sem.at[span, d], pair).wait_recv()

    def ready(t, d):
        tile = t * nchip + part(d)
        value = qraw[t, part(d)].astype(F32)
        qs[tile, :chunk] = jnp.where(lane < hd, value, 0.0).astype(BF16)
        qs[tile, chunk:] = jnp.where(lane < hd, 0.0, value).astype(BF16)

    def needs(t):
        return (core == 1) | (t == 0)

    def take_own(d):
        for t in range(2):
            take(base + held[t], t, d, True)

            @pl.when(needs(t))
            def _():
                fwd(base + held[t], t, 0, d).start()

        for t in range(2):
            ready(t, d)

    def take_own_pair(d):
        for t in range(2):

            @pl.when((core == 0) | (t == 0))
            def _():
                fwd(base + others[t], t, 0, d).wait_recv()

    krow = lax.broadcasted_iota(jnp.int32, (chunk, 2 * chunk), 0)
    qcol = lax.rem(lax.broadcasted_iota(jnp.int32, (chunk, 2 * chunk), 1), chunk)

    def attend(items, diagonal=False):
        scores = []
        for tile, blocks in items:
            row = []
            for span, a in blocks:
                raw = nt(kvb[span, a, :chunk], qs[tile])
                row.append(jnp.where(krow <= qcol, raw, -jnp.inf) if diagonal else raw)
            scores.append(row)
        for (tile, blocks), row in zip(items, scores):
            old = peak[tile]
            top = old
            for raw in row:
                top = jnp.maximum(top, jnp.max(raw, axis=0, keepdims=True))
            rescale = jnp.exp(old - top)
            total = None
            weighted = None
            for (span, a), raw in zip(blocks, row):
                e = jnp.exp(raw - top[:1])
                sums = jnp.sum(e.reshape(chunk // 8, 8, 2 * chunk), axis=0)
                turned = jnp.concatenate(
                    [kvb[span, a, chunk + c * val : chunk + (c + 1) * val] for c in range(chunk // 128)],
                    axis=1)
                got = nn(turned, e.astype(BF16))
                total = sums if total is None else total + sums
                weighted = got if weighted is None else weighted + got
            peak[tile] = top
            den[tile] = den[tile] * rescale + total
            acc[tile] = acc[tile] * rescale[:1] + weighted

    def tile_of(t, d):
        return t * nchip + part(d)

    def whole_slots(i):
        slot_t = jnp.where(core == 0, 1, jnp.minimum(i, 1))
        slot = jnp.where(core == 0, i, jnp.maximum(i - 1, 0))
        return slot_t, slot

    def prior_keys(queries_d, keys_d, fresh):
        @pl.loop(0, g)
        def _(back):
            first = SQUARE * (g - 1 - back)
            for group in range(2):
                slots = held if group == 0 else others
                spans = [first + slots[t] for t in range(2)]
                if fresh:
                    for t in range(2):
                        if group == 0:
                            take(spans[t], t, keys_d, False)
                            fwd(spans[t], t, 1 + back, keys_d).start()
                        else:
                            take(spans[t], t, keys_d, False)
                for e in queries_d:
                    attend([(tile_of(t, e), [(span, part(keys_d)) for span in spans]) for t in range(2)])

    def own_whole(queries_d, keys_d):

        @pl.loop(0, SQUARE - 1)
        def _(i):
            slot_t, slot = whole_slots(i)
            attend([(slot_t * nchip + part(e), [(base + slot, part(keys_d))]) for e in queries_d])

    take_own(0)
    attend([(tile_of(t, 0), [(base + held[t], part(0))]) for t in range(2)], diagonal=True)
    take_own_pair(0)
    own_whole([0], 0)

    for d in range(1, nchip):
        other = part(d)
        for half in range(2):
            landed(other * 2 + core, half)
            to_pair(other * 2 + core, half)
        for half in range(2):
            landed(other * 2 + 1 - core, half)
        project(d)
    for d in range(1, nchip):
        project_ret(d)

    blk = BLOCK
    nblk = rows // blk
    rkw = rheads * hd
    tt = lax.broadcasted_iota(jnp.int32, (blk, blk), 0)
    uu = lax.broadcasted_iota(jnp.int32, (blk, blk), 1)
    rlane = lax.broadcasted_iota(jnp.int32, (blk, rkw), 1)
    srow = lax.broadcasted_iota(jnp.int32, (rkw, val), 0)
    decays = []
    span_state = jnp.zeros((rkw, val), F32)
    span_logs = []
    for h in range(rheads):
        ours = (rlane >= h * hd) & (rlane < (h + 1) * hd)
        keep = (srow >= h * hd) & (srow < (h + 1) * hd)
        state = jnp.zeros((rkw, val), F32)
        log_all = jnp.zeros((1, 1), F32)
        for n in range(nblk):
            at = slice(n * blk, (n + 1) * blk)
            row = log_ref[h : h + 1, at]
            full = jnp.broadcast_to(row, (blk, blk))
            c_col = jnp.sum(jnp.where(uu <= tt, full, 0.0), axis=1, keepdims=True)
            l_col = jnp.sum(jnp.where(uu == tt, full, 0.0), axis=1, keepdims=True)
            c_row = jnp.sum(jnp.where(tt <= uu, l_col, 0.0), axis=0, keepdims=True)
            last = c_col[blk - 1 : blk, :]
            query = jnp.where(ours, rbuf[at, :rkw].astype(F32), 0.0)
            keys = rbuf[at, rkw : 2 * rkw]
            values = rbuf[at, 2 * rkw + h * val : 2 * rkw + (h + 1) * val]
            raw = nt(query.astype(BF16), keys)
            gap = jnp.where(uu <= tt, c_col - c_row, -jnp.inf)
            g_mat = (raw * hd ** (-0.5) * jnp.exp(gap)).astype(BF16)
            rmid[h, at, :] = nn(g_mat, values)
            kd = (keys.astype(F32) * hd ** (-0.5) * jnp.exp(last - c_col)).astype(BF16)
            new = jnp.where(keep, tn(kd, values), 0.0)
            upd[h, n] = new
            state = jnp.exp(last) * state + new
            log_all = log_all + last
            decays.append((c_col, last))
        span_state = span_state + state
        span_logs.append(log_all)
    sts[me, :rkw, :] = span_state.astype(BF16)
    for h in range(rheads):
        wide = jnp.broadcast_to(span_logs[h], (16, val))
        hi = wide.astype(BF16)
        sts[me, rkw + 32 * h : rkw + 32 * h + 16, :] = hi
        sts[me, rkw + 32 * h + 16 : rkw + 32 * h + 32, :] = (wide - hi.astype(F32)).astype(BF16)

    @pl.when(first_up)
    def _():
        st_copy(0, me, sem_zs, up).start()

    @pl.when(b == 0)
    def _():
        st_copy(0, me, sem_ys, side).start()

    prior_keys([0], 0, True)
    relay(1)

    for d in range(1, nchip):
        take_own(d)
        if d == 1 and npair > 2:
            relay(2)
        for e in range(d):
            prior_keys([d], e, False)
            own_whole([d], e)
            high = jnp.maximum(part(d), part(e))
            low = jnp.minimum(part(d), part(e))
            attend([(t * nchip + high, [(base + held[t], low)]) for t in range(2)])
        attend([(tile_of(t, d), [(base + held[t], part(d))]) for t in range(2)], diagonal=True)
        take_own_pair(d)
        own_whole(list(range(d + 1)), d)
        if d == 1:

            @pl.loop(3, npair)
            def _(i):
                relay(i)

            first = []
            for h in range(rheads):
                parts = ([jnp.zeros((hd, val), F32)] * h + [init_ref[h]]
                         + [jnp.zeros((hd, val), F32)] * (rheads - 1 - h))
                first.append(jnp.concatenate(parts, axis=0) if rheads > 1 else parts[0])

            @pl.loop(1, npair + 1)
            def _(i):
                jy = 2 * (p - i + 1) + 1 - b

                @pl.when((i - 1 <= p) & ((b == 1) | (i > 1)))
                def _():
                    st_copy(i, jy, sem_ys, side).wait_recv()

            def join(j, states):
                out = []
                for h in range(rheads):
                    keep = (srow >= h * hd) & (srow < (h + 1) * hd)
                    low = rkw + 32 * h
                    log = sts[j, low : low + 16, :].astype(F32) + sts[j, low + 16 : low + 32, :].astype(F32)
                    piece = jnp.where(keep, sts[j, :rkw, :].astype(F32), 0.0)
                    out.append(jnp.exp(log[:1, :]) * states[h] + piece)
                return tuple(out)

            carried = lax.fori_loop(0, me, join, tuple(first))
            for h in range(rheads):
                state = carried[h]
                for n in range(nblk):
                    at = slice(n * blk, (n + 1) * blk)
                    c_col, last = decays[h * nblk + n]
                    query = rbuf[at, :rkw].astype(F32) * jnp.exp(c_col)
                    result = rmid[h, at, :] + nn(query, state, precision=HIGHEST)
                    if n + 1 < nblk:
                        state = jnp.exp(last) * state + upd[h, n]
                    mixr[at, h * val : (h + 1) * val] = head_norm(result).astype(BF16)
        prior_keys(list(range(d + 1)), d, True)

    lam_copy(1 - core).wait_recv()
    lam = lamv[head_core, pl.ds(pl.multiple_of(8 * head_no, 8), 8), :][:1, :1]

    def d_copy(t, d):
        where = {"sp": base + held[t], "tp": chip * 2 + head_core}
        return remote(dsend.at[t, part(d)], dret.at[head_no, part(d)], ds_sem.at[t, d],
                      rd_sem.at[head_no, d], where)

    def d_local(t, d):
        return pltpu.make_async_copy(dsend.at[t, part(d)], dret.at[head_no, part(d)],
                                     rd_sem.at[head_no, d])

    def home(t):
        return (held[t] == s) & (head_core == core)

    targets = list(range(1, nchip)) + [0]
    for d in targets:
        for t in range(2):
            tile = tile_of(t, d)
            scale = 1.0 / jnp.sum(den[tile], axis=0, keepdims=True)
            out = acc[tile] * scale
            merged = out[:, :chunk] - lam * out[:, chunk:]
            square = jnp.mean(merged * merged, axis=0, keepdims=True)
            normed = (merged * lax.rsqrt(square + HEAD_EPS)).T
            dsend[t, part(d)] = (normed * gain_ref[...] * DIFF_SCALE).astype(BF16)

            @pl.when(home(t))
            def _():
                d_local(t, d).start()

            @pl.when(jnp.logical_not(home(t)))
            def _():
                d_copy(t, d).start()

    for load in out_loads:
        load.wait()

    width = out_ref.shape[1]
    cut = mine.shape[2]
    npiece = width // cut

    def returned(d):
        for h in range(heads):
            here = stays(h)

            @pl.when(here)
            def _():
                d_local(0, d).wait()

            @pl.when(jnp.logical_not(here))
            def _():
                remote(dret.at[h, part(d)], dret.at[h, part(d)], ds_sem.at[0, d], rd_sem.at[h, d],
                       pair).wait_recv()

    def partial(which, half, n):
        inner = pl.ds(pl.multiple_of(half * own_rows, own_rows), own_rows)
        owner = which * 2 + half
        rest = mixr[pl.ds(pl.multiple_of(owner * own_rows, own_rows), own_rows), :]
        left = jnp.concatenate([dret[h, which, inner, :] for h in range(heads)] + [rest], axis=1)
        return nn(left, wobuf[:, n * cut : (n + 1) * cut])

    def pair_copy(d, n):
        return remote(mine.at[d * npiece + n], from_pair.at[d * npiece + n], mpair_send.at[d, n],
                      mpair_recv.at[d, n], pair)

    def chip_copy(d, n):
        there = lax.rem(chip + d, nchip) * 2 + core
        return remote(sent.at[d * npiece + n], from_chip.at[d * npiece + n], mchip_send.at[d, n],
                      mchip_recv.at[d, n], {"tp": there})

    for d in targets:
        which = lax.rem(chip + d, nchip)
        returned((nchip - d) % nchip)
        for n in range(npiece):
            mine[d * npiece + n] = partial(which, 1 - core, n).astype(BF16)
            pair_copy(d, n).start()
        if d:
            for n in range(npiece):
                ours = partial(which, core, n)
                pair_copy(d, n).wait_recv()
                sent[d * npiece + n] = (ours + from_pair[d * npiece + n].astype(F32)).astype(BF16)
                chip_copy(d, n).start()
    for n in range(npiece):
        total = partial(chip, core, n)
        pair_copy(0, n).wait_recv()
        total = total + from_pair[n].astype(F32)
        for d in range(1, nchip):
            chip_copy(d, n).wait_recv()
            total = total + from_chip[d * npiece + n].astype(F32)
        out_ref[:, n * cut : (n + 1) * cut] = total.astype(BF16)

    for copy in copies:
        copy.wait_send()

    for d in range(nchip):
        for h in range(heads):

            @pl.when(jnp.logical_not(stays(h)))
            def _():
                q_copy(h, d).wait_send()
                kv_copy(h, d, 0).wait_send()

        for dg in range(1, ngroup):

            @pl.when(g + dg < ngroup)
            def _():
                for h in range(heads):
                    kv_copy(h, d, dg).wait_send()

        for t in range(2):

            @pl.when(needs(t))
            def _():
                fwd(base + held[t], t, 0, d).wait_send()

            @pl.when(jnp.logical_not(home(t)))
            def _():
                d_copy(t, d).wait_send()

        @pl.loop(0, g)
        def _(back):
            for t in range(2):
                fwd(SQUARE * (g - 1 - back) + held[t], t, 1 + back, d).wait_send()

    @pl.loop(0, npair)
    def _(i):
        j = 2 * (p - i) + b

        @pl.when((i <= p) & first_up)
        def _():
            st_copy(i, j, sem_zs, up).wait_send()

        @pl.when((i <= p) & ((i > 0) | (b == 0)))
        def _():
            st_copy(i, j, sem_ys, side).wait_send()

    for d in targets:
        for n in range(npiece):
            pair_copy(d, n).wait_send()
            if d:
                chip_copy(d, n).wait_send()


VMEM = pl.BlockSpec(memory_space=pltpu.VMEM)
ANY = pl.BlockSpec(memory_space=pl.ANY)
SMEM = pl.BlockSpec(memory_space=pltpu.SMEM)
DMA = pltpu.SemaphoreType.DMA


def params(number):
    return pltpu.CompilerParams(
        collective_id=number, has_side_effects=True, vmem_limit_bytes=VMEM_LIMIT
    )


def on_device(nsp, ntp, tokens, norm_gain, w_query_one, w_query_two, w_key_one, w_key_two, w_value,
              mix_lambda, head_gain, w_ret_query, w_ret_key, w_ret_value, retain_log, init_state,
              w_out_diff, w_out_ret):
    weights = (w_query_one, w_query_two, w_key_one, w_key_two, w_value, w_ret_query, w_ret_key, w_ret_value)
    widths = tuple(w.shape[1] for w in weights)
    own_rows, model = tokens.shape
    rows = own_rows * ntp
    nchip = ntp // 2
    npair = nsp // 2
    ngroup = nsp // SQUARE
    chunk = rows // nchip
    heads = mix_lambda.shape[0]
    rheads, hd, val = init_state.shape
    kw = widths[2]
    width = w_out_diff.shape[1]
    npiece = 4
    cut = width // npiece
    return pl.pallas_call(
        functools.partial(layer_kernel, nsp, ntp, widths, heads, rheads),
        out_shape=jax.ShapeDtypeStruct((own_rows, width), BF16),
        in_specs=[SMEM] + [VMEM] * 5 + [ANY] * (len(weights) + 2),
        out_specs=VMEM,
        scratch_shapes=[
            pltpu.VMEM((ntp, own_rows, model), BF16),
            pltpu.VMEM((model, sum(widths)), BF16),
            pltpu.VMEM((w_out_diff.shape[0] + w_out_ret.shape[0], width), BF16),
            pltpu.VMEM((heads, nchip, chunk, kw), BF16),
            pltpu.VMEM((heads, nchip, 2 * chunk, kw), BF16),
            pltpu.VMEM((nsp, nchip, 2 * chunk, kw), BF16),
            pltpu.VMEM((2, nchip, chunk, kw), BF16),
            pltpu.VMEM((2 * nchip, 2 * chunk, kw), BF16),
            pltpu.VMEM((2, 8 * heads, 128), F32),
            pltpu.VMEM((2 * nchip, 8, 2 * chunk), F32),
            pltpu.VMEM((2 * nchip, 8, 2 * chunk), F32),
            pltpu.VMEM((2 * nchip, val, 2 * chunk), F32),
            pltpu.VMEM((2, nchip, chunk, val), BF16),
            pltpu.VMEM((heads, nchip, chunk, val), BF16),
            pltpu.VMEM((nsp, rheads * hd + 32 * rheads, val), BF16),
            pltpu.VMEM((rows, sum(widths[5:])), BF16),
            pltpu.VMEM((rheads, rows, val), F32),
            pltpu.VMEM((rheads, rows // BLOCK, rheads * hd, val), F32),
            pltpu.VMEM((rows, rheads * val), BF16),
            pltpu.VMEM((nchip * npiece, own_rows, cut), BF16),
            pltpu.VMEM((nchip * npiece, own_rows, cut), BF16),
            pltpu.VMEM((nchip * npiece, own_rows, cut), BF16),
            pltpu.VMEM((nchip * npiece, own_rows, cut), BF16),
            DMA((len(weights) + 2,)),
            DMA((2,)),
            DMA((nchip, 2)),
            DMA((nchip, 2)),
            DMA((ntp, 2)),
            DMA((heads, nchip)),
            DMA((heads, nchip)),
            DMA((max(ngroup - 1, 1), heads, nchip)),
            DMA((ngroup, 2, nchip)),
            DMA((2, nchip)),
            DMA((nsp, nchip)),
            DMA((2, nchip)),
            DMA((heads, nchip)),
            DMA((npair + 1,)),
            DMA((npair + 1,)),
            DMA((nsp,)),
            DMA((nchip, npiece)),
            DMA((nchip, npiece)),
            DMA((nchip, npiece)),
            DMA((nchip, npiece)),
        ],
        compiler_params=params(0),
        name="layer",
    )(mix_lambda, tokens, norm_gain[None, :], head_gain[None, :], retain_log, init_state, *weights,
      w_out_diff, w_out_ret)


def solution(mesh):
    in_specs = (
        P(("sp", "tp"), None),
        P(),
        P(None, "tp"),
        P(None, "tp"),
        P(None, "tp"),
        P(None, "tp"),
        P(None, "tp"),
        P("tp"),
        P(),
        P(None, "tp"),
        P(None, "tp"),
        P(None, "tp"),
        P("tp", "sp"),
        P("tp", None, None),
        P("tp", None),
        P("tp", None),
    )
    body = functools.partial(on_device, mesh.shape["sp"], mesh.shape["tp"])
    return jax.shard_map(
        body, mesh=mesh, in_specs=in_specs, out_specs=P(("sp", "tp"), None), check_vma=False
    )
```

```python
import functools

import jax
import jax.numpy as jnp
from jax import lax
from jax.experimental import pallas as pl
from jax.experimental.pallas import tpu as pltpu
from jax.sharding import PartitionSpec as P

BLOCK = 256
SQUARE = 4
NORM_EPS = 1e-06
HEAD_EPS = 1e-05
DIFF_SCALE = 0.8
HIGHEST = lax.Precision.HIGHEST
MESH = pl.DeviceIdType.MESH
F32 = jnp.float32
BF16 = jnp.bfloat16
VMEM_LIMIT = 60 * 1024 * 1024


def remote(src, dst, send, recv, where):
    return pltpu.make_async_remote_copy(
        src_ref=src, dst_ref=dst, send_sem=send, recv_sem=recv,
        device_id=where, device_id_type=MESH,
    )


def scoped(name):
    def wrap(step):
        def run(*args, **kw):
            with jax.named_scope(name):
                return step(*args, **kw)
        return run
    return wrap


def head_norm(values):
    return values * lax.rsqrt(jnp.mean(values * values, axis=-1, keepdims=True) + HEAD_EPS)


def nn(a, b, **kw):
    return lax.dot_general(a, b, (((1,), (0,)), ((), ())), preferred_element_type=F32, **kw)


def nt(a, b):
    return lax.dot_general(a, b, (((1,), (1,)), ((), ())), preferred_element_type=F32)


def tn(a, b):
    return lax.dot_general(a, b, (((0,), (0,)), ((), ())), preferred_element_type=F32)


def layer_kernel(nsp, ntp, widths, heads, rheads, lam_ref, tokens_ref, ngain_ref, gain_ref, log_ref,
                 init_ref, *refs):
    nw = len(widths)
    w_refs = refs[:nw]
    wd_ref, wr_ref, out_ref = refs[nw : nw + 3]
    (gat, wbuf, wobuf, wx, sndq, sndkv, kvb, qraw, qs, lamv, peak, den, acc, dsend, dret, sts, rbuf,
     decay, along, rmid, upd, mixr, mine, sent, from_pair, from_chip, wsem, lsem, pair_send, cross_send,
     grecv, wx_send, wx_side, wx_recv, sq_sem, skv_sem, inter_sem, fwd_sem, rq_sem, rkv_sem, ds_sem,
     rd_sem, st_send, st_up, st_on, st_recv, mpair_send, mpair_recv, mchip_send, mchip_recv) = refs[nw + 3 :]
    me = lax.axis_index("sp")
    b = lax.rem(me, 2)
    ngroup = nsp // SQUARE
    g = me // SQUARE
    s = lax.rem(me, SQUARE)
    side = {"sp": me + 1 - 2 * b}
    tme = lax.axis_index("tp")
    core = lax.rem(tme, 2)
    chip = tme // 2
    nchip = ntp // 2
    tpair = tme + 1 - 2 * core
    pair = {"tp": tpair}
    own_rows = tokens_ref.shape[0]
    rows = own_rows * ntp
    chunk = rows // nchip
    kw = widths[2]
    hd = kw // heads
    val = gain_ref.shape[1]

    held = (core, SQUARE - 1 - core)
    others = (1 - core, 2 + core)
    land = lax.rem((s + 1) // 2, 2)
    head_core = s // 2
    head_no = lax.rem(s, 2)
    base = SQUARE * g

    barrier = pltpu.get_barrier_semaphore()

    def greet(where):
        pl.semaphore_signal(barrier, inc=1, device_id=where, device_id_type=MESH)

    for k in range(1, ntp):
        greet({"tp": lax.rem(tme + k, ntp)})
    for k in range(1, SQUARE):
        for n in range(ntp):
            greet({"sp": base + lax.rem(s + k, SQUARE), "tp": n})
    for dg in range(1, ngroup):

        @pl.when(g + dg < ngroup)
        def _():
            for h in range(2):
                greet({"sp": base + SQUARE * dg + 2 * core + h, "tp": chip * 2 + land})
            greet({"sp": me + SQUARE * dg})

        @pl.when(g >= dg)
        def _():
            for t in range(2):
                greet({"sp": base - SQUARE * dg + held[t], "tp": chip * 2 + head_core})
            greet({"sp": me - SQUARE * dg})

    order = (0, 1, 2, 3, 4, 5, 6, 7)
    starts = [sum(widths[:n]) for n in range(nw)]
    loads = {}
    for n in order:
        at = starts[n]
        loads[n] = pltpu.make_async_copy(w_refs[n], wbuf.at[:, at : at + widths[n]], wsem.at[n])
        loads[n].start()
    depth = wd_ref.shape[0]
    out_loads = [
        pltpu.make_async_copy(wd_ref, wobuf.at[:depth], wsem.at[nw]),
        pltpu.make_async_copy(wr_ref, wobuf.at[depth:], wsem.at[nw + 1]),
    ]
    for load in out_loads:
        load.start()
    floats = tokens_ref[...].astype(F32)
    gat[tme] = (
        floats * lax.rsqrt(jnp.mean(floats * floats, axis=-1, keepdims=True) + NORM_EPS) * ngain_ref[...]
    ).astype(BF16)
    for h in range(heads):
        lamv[core, 8 * h : 8 * h + 8, :] = jnp.full((8, 128), lam_ref[h], F32)
    pl.semaphore_wait(barrier, (ntp - 1) + (SQUARE - 1) * ntp + 3 * (ngroup - 1))
    copies = []

    def begin(copy):
        copies.append(copy)
        copy.start()

    def slab(which, half):
        return gat.at[which, pl.ds(half * (own_rows // 2), own_rows // 2)]

    def crossing():
        for d in range(1, nchip):
            there = {"tp": lax.rem(chip + d, nchip) * 2 + core}
            for half in range(2):
                yield remote(slab(tme, half), slab(tme, half), cross_send.at[d, half],
                             grecv.at[tme, half], there)

    def cross(which):
        @pl.when(core == which)
        def _():
            for copy in crossing():
                copy.start()

    cross(0)
    copies.extend(crossing())

    def pair_slab(which, half):
        return remote(slab(which, half), slab(which, half), pair_send.at[which // 2, half],
                      grecv.at[which, half], pair)

    @scoped("landed")
    def landed(which, half):
        remote(slab(which, half), slab(which, half), pair_send.at[which // 2, half],
               grecv.at[which, half], pair).wait_recv()

    def lam_copy(who):
        return remote(lamv.at[who], lamv.at[who], lsem.at[0], lsem.at[1], pair)

    def part(d):
        return lax.rem(chip + nchip - d, nchip)

    def keys_at(d):
        return pl.ds(pl.multiple_of(part(d) * chunk, chunk), chunk)

    def steps(d):
        return ((0, 0, 2),) if d == 0 else ((2 * d - 1, 0, 1), (2 * d, 1, 1))

    def q_rows(ref, at, step):
        return ref.at[at, pl.ds(step[1] * own_rows, step[2] * own_rows)]

    def kv_rows(ref, at, step):
        return ref.at[at, pl.ds(step[1] * 2 * own_rows, step[2] * 2 * own_rows)]

    def q_copy(h, d, step):
        where = {"sp": base + 2 * core + h, "tp": chip * 2 + land}
        return remote(q_rows(sndq.at[h], part(d), step), q_rows(qraw.at[s // 2], part(d), step),
                      sq_sem.at[h, step[0]], rq_sem.at[s // 2, d], where)

    def kv_copy(h, d, dg, step):
        where = {"sp": base + SQUARE * dg + 2 * core + h, "tp": chip * 2 + land}
        sem = skv_sem.at[h, step[0]] if dg == 0 else inter_sem.at[dg - 1, h, step[0]]
        return remote(kv_rows(sndkv.at[h], part(d), step), kv_rows(kvb.at[me], part(d), step), sem,
                      rkv_sem.at[me, d], where)

    def q_local(h, d, step):
        return pltpu.make_async_copy(q_rows(sndq.at[h], part(d), step),
                                     q_rows(qraw.at[s // 2], part(d), step), rq_sem.at[s // 2, d])

    def kv_local(h, d, step):
        return pltpu.make_async_copy(kv_rows(sndkv.at[h], part(d), step),
                                     kv_rows(kvb.at[me], part(d), step), rkv_sem.at[me, d])

    def stays(h):
        return (2 * core + h == s) & (land == core)

    def fwd(span, t, dg, d):
        piece = kvb.at[span, part(d)]
        return remote(piece, piece, fwd_sem.at[dg, t, d], rkv_sem.at[span, d], pair)

    lane = lax.broadcasted_iota(jnp.int32, (chunk, 128), 1)

    @scoped("project")
    def project(d, step):
        number, first, slabs = step
        count = slabs * own_rows
        rows_in = gat[pl.ds(part(d) * 2 + first, slabs)].reshape(count, gat.shape[2])
        low = lane[:count] < hd

        def product(lo, hi):
            if d == 0:
                for n in range(lo, hi):
                    loads[n].wait()
            span = sum(widths[lo:hi])
            return nn(rows_in, wbuf[:, starts[lo] : starts[lo] + span]).astype(BF16).astype(F32)

        def by_head(pairs):
            one, two = pairs[:, :kw], pairs[:, kw:]
            return (jnp.where(low, one, pltpu.roll(two, hd, 1)),
                    jnp.where(low, pltpu.roll(one, kw - hd, 1), two))

        queries = by_head(product(0, 2) * hd ** (-0.5))
        for h in range(heads):
            sndq[h, part(d), first * own_rows : first * own_rows + count] = queries[h].astype(BF16)
        keys = by_head(product(2, 4))
        values = product(4, 5)
        for h in range(heads):
            turned = values[:, h * val : (h + 1) * val].T.astype(BF16)
            for c in range(slabs):
                at = 2 * own_rows * (first + c)
                rows_of = slice(c * own_rows, (c + 1) * own_rows)
                sndkv[h, part(d), at : at + own_rows] = keys[h][rows_of].astype(BF16)
                sndkv[h, part(d), at + own_rows : at + 2 * own_rows] = turned[:, rows_of]
        for h in range(heads):

            @pl.when(stays(h))
            def _():
                q_local(h, d, step).start()
                kv_local(h, d, step).start()

            @pl.when(jnp.logical_not(stays(h)))
            def _():
                q_copy(h, d, step).start()
                kv_copy(h, d, 0, step).start()

    def to_later(d, step, only=None):
        for dg in range(1, ngroup):
            goes = g + dg < ngroup
            if only is not None:
                goes = goes & (core == only)

            @pl.when(goes)
            def _():
                for h in range(heads):
                    kv_copy(h, d, dg, step).start()

    @scoped("project_ret")
    def project_ret(d):
        both = gat[pl.ds(part(d) * 2, 2)].reshape(chunk, gat.shape[2])
        if d == 0:
            for n in range(5, 8):
                loads[n].wait()
        span = sum(widths[5:8])
        for c in range(0, span, 256):
            rbuf[keys_at(d), c : c + 256] = nn(
                both, wbuf[:, starts[5] + c : starts[5] + c + 256]).astype(BF16)

    wpiece = depth // 4

    def w_rows(ref, half, n):
        return ref.at[pl.ds(pl.multiple_of(half * 2 * wpiece, 2 * wpiece) + n * wpiece, wpiece)]

    def w_cross(d, n):
        there = {"tp": lax.rem(chip + d, nchip) * 2 + core}
        return remote(w_rows(wobuf, b, n), w_rows(wx.at[nchip - d - 1], b, n), wx_send.at[d - 1, n],
                      wx_recv.at[nchip - d - 1, b, n], there)

    def w_side(d, half, n):
        piece = w_rows(wx.at[d - 1], half, n)
        return remote(piece, piece, wx_side.at[d - 1, n], wx_recv.at[d - 1, half, n], side)

    @scoped("w_pass")
    def w_pass(n):
        for d in range(1, nchip):
            w_side(d, b, n).wait_recv()
            w_side(d, b, n).start()

    for half in range(2):
        begin(pair_slab(tme, half))
    for d in range(1, nchip):
        for half in range(2):
            copies.append(pair_slab(part(d) * 2 + core, half))
    begin(lam_copy(core))
    peak[...] = jnp.full(peak.shape, -jnp.inf, F32)
    den[...] = jnp.zeros(den.shape, F32)
    acc[...] = jnp.zeros(acc.shape, F32)
    for half in range(2):
        landed(tpair, half)
    project(0, steps(0)[0])
    to_later(0, steps(0)[0])
    cross(1)
    project_ret(0)

    blk = BLOCK
    nblk = rows // blk
    rkw = rheads * hd
    tt = lax.broadcasted_iota(jnp.int32, (blk, blk), 0)
    uu = lax.broadcasted_iota(jnp.int32, (blk, blk), 1)
    rlane = lax.broadcasted_iota(jnp.int32, (blk, rkw), 1)
    srow = lax.broadcasted_iota(jnp.int32, (rkw, val), 0)

    def ours(iota, h):
        return (iota >= h * hd) & (iota < (h + 1) * hd)

    @scoped("decays")
    def decays():
        for h in range(rheads):
            for n in range(nblk):
                row = log_ref[h : h + 1, n * blk : (n + 1) * blk]
                full = jnp.broadcast_to(row, (blk, blk))
                c_col = jnp.sum(jnp.where(uu <= tt, full, 0.0), axis=1, keepdims=True)
                l_col = jnp.sum(jnp.where(uu == tt, full, 0.0), axis=1, keepdims=True)
                c_row = jnp.sum(jnp.where(tt <= uu, l_col, 0.0), axis=0, keepdims=True)
                decay[h, n] = jnp.exp(jnp.where(uu <= tt, c_col - c_row, -jnp.inf))
                along[h, n] = jnp.broadcast_to(c_col, (blk, 128))

    def blocks_of(d):
        for i in range(chunk // blk):
            n = part(d) * (chunk // blk) + i
            yield n, pl.ds(pl.multiple_of(n * blk, blk), blk)

    @scoped("ret_states")
    def ret_states(d):
        for n, at in blocks_of(d):
            keys = rbuf[at, rkw : 2 * rkw].astype(F32) * hd ** (-0.5)
            for h in range(rheads):
                c = along[h, n]
                kd = (keys * jnp.exp(c[blk - 1 : blk, :1] - c[:, :1])).astype(BF16)
                values = rbuf[at, 2 * rkw + h * val : 2 * rkw + (h + 1) * val]
                upd[h, n] = jnp.where(ours(srow, h), tn(kd, values), 0.0)

    @scoped("ret_inner")
    def ret_inner(d):
        for n, at in blocks_of(d):
            keys = rbuf[at, rkw : 2 * rkw]
            for h in range(rheads):
                query = jnp.where(ours(rlane, h), rbuf[at, :rkw].astype(F32), 0.0)
                raw = nt(query.astype(BF16), keys)
                weights = (raw * hd ** (-0.5) * decay[h, n]).astype(BF16)
                rmid[h, at, :] = nn(weights, rbuf[at, 2 * rkw + h * val : 2 * rkw + (h + 1) * val])

    logrow = lax.broadcasted_iota(jnp.int32, (16, val), 0)

    def put_state(slot, state, logs):
        sts[slot, :rkw, :] = state.astype(BF16)
        tile = jnp.zeros((16, val), F32)
        for h in range(rheads):
            wide = jnp.broadcast_to(logs[h], (16, val))
            hi = wide.astype(BF16).astype(F32)
            tile = jnp.where(logrow == 2 * h, hi, tile)
            tile = jnp.where(logrow == 2 * h + 1, wide - hi, tile)
        sts[slot, rkw:, :] = tile.astype(BF16)

    def join(slot, states):
        piece = sts[slot, :rkw, :].astype(F32)
        logs = sts[slot, rkw:, :].astype(F32)
        return tuple(
            jnp.exp(logs[2 * h : 2 * h + 1] + logs[2 * h + 1 : 2 * h + 2]) * states[h]
            + jnp.where(ours(srow, h), piece, 0.0)
            for h in range(rheads)
        )

    def st_copy(k):
        return remote(sts.at[me], sts.at[me], st_send.at[k], st_recv.at[me],
                      {"sp": base + lax.rem(s + k, SQUARE)})

    def st_later(dg):
        return remote(sts.at[me], sts.at[me], st_up.at[dg], st_recv.at[me], {"sp": me + SQUARE * dg})

    def st_pass(back, k):
        span = me - SQUARE * (back + 1)
        return remote(sts.at[span], sts.at[span], st_on.at[back, k], st_recv.at[span],
                      {"sp": base + lax.rem(s + k, SQUARE)})

    def st_wait(span):
        remote(sts.at[span], sts.at[span], st_send.at[0], st_recv.at[span], pair).wait_recv()

    @scoped("span_state")
    def span_state():
        total = jnp.zeros((rkw, val), F32)
        logs = []
        for h in range(rheads):
            state = jnp.zeros((rkw, val), F32)
            log_all = jnp.zeros((1, 1), F32)
            for n in range(nblk):
                last = along[h, n, blk - 1 : blk, :1]
                state = jnp.exp(last) * state + upd[h, n]
                log_all = log_all + last
            total = total + state
            logs.append(log_all)
        put_state(me, total, logs)
        for k in range(1, SQUARE):

            @pl.when(s + k < SQUARE)
            def _():
                st_copy(k).start()

        for dg in range(1, ngroup):

            @pl.when(g + dg < ngroup)
            def _():
                st_later(dg).start()

    @scoped("pass_states")
    def pass_states():
        @pl.loop(0, g)
        def _(back):
            st_wait(me - SQUARE * (back + 1))
            for k in range(1, SQUARE):
                st_pass(back, k).start()

    @scoped("ret_finish")
    def ret_finish():
        first = []
        for h in range(rheads):
            parts = ([jnp.zeros((hd, val), F32)] * h + [init_ref[h]]
                     + [jnp.zeros((hd, val), F32)] * (rheads - 1 - h))
            first.append(jnp.concatenate(parts, axis=0) if rheads > 1 else parts[0])

        @pl.loop(0, g)
        def _(back):
            for k in range(1, SQUARE):
                st_wait(base - SQUARE * (back + 1) + lax.rem(s + k, SQUARE))

        @pl.loop(0, s)
        def _(slot):
            st_wait(base + slot)

        carried = lax.fori_loop(0, me, join, tuple(first))
        for h in range(rheads):
            state = carried[h]
            for n in range(nblk):
                at = slice(n * blk, (n + 1) * blk)
                c = along[h, n]
                query = rbuf[at, :rkw].astype(F32) * jnp.exp(c[:, :1])
                result = rmid[h, at, :] + nn(query, state, precision=HIGHEST)
                if n + 1 < nblk:
                    state = jnp.exp(c[blk - 1 : blk, :1]) * state + upd[h, n]
                mixr[at, h * val : (h + 1) * val] = head_norm(result).astype(BF16)

    decays()
    ret_states(0)
    ret_inner(0)

    @scoped("take")
    def take(span, t, d, local):
        if local:
            here = (held[t] == s) & (head_core == core)

            @pl.when(here)
            def _():
                pltpu.make_async_copy(sndq.at[0, part(d)], qraw.at[t, part(d)], rq_sem.at[t, d]).wait()
                pltpu.make_async_copy(sndkv.at[0, part(d)], kvb.at[span, part(d)],
                                      rkv_sem.at[span, d]).wait()

            @pl.when(jnp.logical_not(here))
            def _():
                remote(qraw.at[t, part(d)], qraw.at[t, part(d)], sq_sem.at[0, d],
                       rq_sem.at[t, d], pair).wait_recv()
                remote(kvb.at[span, part(d)], kvb.at[span, part(d)], skv_sem.at[0, d],
                       rkv_sem.at[span, d], pair).wait_recv()
        else:
            remote(kvb.at[span, part(d)], kvb.at[span, part(d)], skv_sem.at[0, d],
                   rkv_sem.at[span, d], pair).wait_recv()

    def ready(t, d):
        tile = t * nchip + part(d)
        value = qraw[t, part(d)].astype(F32)
        qs[tile, :chunk] = jnp.where(lane < hd, value, 0.0).astype(BF16)
        qs[tile, chunk:] = jnp.where(lane < hd, 0.0, value).astype(BF16)

    def needs(t):
        return (core == 1) | (t == 0)

    def take_own(d):
        for t in range(2):
            take(base + held[t], t, d, True)

            @pl.when(needs(t))
            def _():
                fwd(base + held[t], t, 0, d).start()

        for t in range(2):
            ready(t, d)

    @scoped("take_own_pair")
    def take_own_pair(d):
        for t in range(2):

            @pl.when((core == 0) | (t == 0))
            def _():
                fwd(base + others[t], t, 0, d).wait_recv()

    krow = lax.broadcasted_iota(jnp.int32, (chunk, 2 * chunk), 0)
    qcol = lax.rem(lax.broadcasted_iota(jnp.int32, (chunk, 2 * chunk), 1), chunk)

    @scoped("attend")
    def attend(items, diagonal=False):
        scores = []
        for tile, blocks in items:
            row = []
            for span, a in blocks:
                keys = jnp.concatenate(
                    [kvb[span, a, 2 * c * own_rows : (2 * c + 1) * own_rows] for c in range(2)], axis=0)
                raw = nt(keys, qs[tile])
                row.append(jnp.where(krow <= qcol, raw, -jnp.inf) if diagonal else raw)
            scores.append(row)
        for (tile, blocks), row in zip(items, scores):
            old = peak[tile]
            top = old
            for raw in row:
                top = jnp.maximum(top, jnp.max(raw, axis=0, keepdims=True))
            rescale = jnp.exp(old - top)
            total = None
            weighted = None
            for (span, a), raw in zip(blocks, row):
                e = jnp.exp(raw - top[:1])
                sums = jnp.sum(e.reshape(chunk // 8, 8, 2 * chunk), axis=0)
                turned = jnp.concatenate(
                    [kvb[span, a, (2 * c + 1) * own_rows : (2 * c + 2) * own_rows] for c in range(2)],
                    axis=1)
                got = nn(turned, e.astype(BF16))
                total = sums if total is None else total + sums
                weighted = got if weighted is None else weighted + got
            peak[tile] = top
            den[tile] = den[tile] * rescale + total
            acc[tile] = acc[tile] * rescale[:1] + weighted

    def tile_of(t, d):
        return t * nchip + part(d)

    def prior_keys(queries_d, keys_d, fresh):
        @pl.loop(0, g)
        def _(back):
            first = SQUARE * (g - 1 - back)
            for group in range(2):
                slots = held if group == 0 else others
                spans = [first + slots[t] for t in range(2)]
                if fresh:
                    for t in range(2):
                        if group == 0:
                            take(spans[t], t, keys_d, False)
                            fwd(spans[t], t, 1 + back, keys_d).start()
                        else:
                            take(spans[t], t, keys_d, False)
                for e in queries_d:
                    attend([(tile_of(t, e), [(span, part(keys_d)) for span in spans]) for t in range(2)])

    def own_whole(queries_d, keys_d):
        third_t, third_slot = 1 - core, 2 * (1 - core)
        at = part(keys_d)
        attend([item for e in queries_d for item in (
            (nchip + part(e), ((base, at), (base + 1, at))),
            (third_t * nchip + part(e), ((base + third_slot, at),)),
        )])

    width = out_ref.shape[1]
    cut = mine.shape[2]
    npiece = width // cut

    def mixed_rows(which, half):
        owner = which * 2 + half
        return mixr[pl.ds(pl.multiple_of(owner * own_rows, own_rows), own_rows), :]

    def pair_copy(d, n):
        return remote(mine.at[d * npiece + n], from_pair.at[d * npiece + n], mpair_send.at[d, n],
                      mpair_recv.at[d, n], pair)

    def chip_copy(d, n):
        there = lax.rem(chip + d, nchip) * 2 + core
        return remote(sent.at[d * npiece + n], from_chip.at[d * npiece + n], mchip_send.at[d, n],
                      mchip_recv.at[d, n], {"tp": there})

    @scoped("ret_reduce")
    def ret_reduce():
        out_loads[1].wait()
        for d in range(1, nchip):
            which = lax.rem(chip + d, nchip)
            for n in range(npiece):
                cols = wobuf[depth:, n * cut : (n + 1) * cut]
                mine[d * npiece + n] = nn(mixed_rows(which, 1 - core), cols).astype(BF16)
                pair_copy(d, n).start()

    @scoped("ret_send")
    def ret_send():
        for d in range(1, nchip):
            which = lax.rem(chip + d, nchip)
            for n in range(npiece):
                cols = wobuf[depth:, n * cut : (n + 1) * cut]
                part_sum = nn(mixed_rows(which, core), cols)
                pair_copy(d, n).wait_recv()
                sent[d * npiece + n] = (part_sum + from_pair[d * npiece + n].astype(F32)).astype(BF16)
                chip_copy(d, n).start()

    def slab_in(d, which):
        index = part(d) * 2 + which
        for half in range(2):
            landed(index, half)

            @pl.when(core == which)
            def _():
                pair_slab(index, half).start()

    for d in range(1, nchip):
        slab_in(d, 0)
        project(d, steps(d)[0])
        to_later(d, steps(d)[0], 0)

    take_own(0)
    attend([(tile_of(t, 0), [(base + held[t], part(0))]) for t in range(2)], diagonal=True)
    take_own_pair(0)
    own_whole([0], 0)

    for d in range(1, nchip):
        slab_in(d, 1)
        if d == nchip - 1:
            out_loads[0].wait()
            for e in range(1, nchip):
                for n in range(2):
                    w_cross(e, n).start()
        project_ret(d)
        ret_states(d)
        if d == nchip - 1:
            span_state()
        project(d, steps(d)[1])
        to_later(d, steps(d)[1], 0)
        if d < nchip - 1:
            for step in steps(d):
                to_later(d, step, 1)
        ret_inner(d)
    prior_keys([0], 0, True)
    pass_states()

    for d in range(1, nchip):
        take_own(d)
        if d == nchip - 1:
            w_pass(0)
            ret_finish()
            ret_reduce()
            w_pass(1)
            ret_send()
            for step in steps(d):
                to_later(d, step, 1)
        for e in range(d):
            prior_keys([d], e, False)
            own_whole([d], e)
            high = jnp.maximum(part(d), part(e))
            low = jnp.minimum(part(d), part(e))
            attend([(t * nchip + high, [(base + held[t], low)]) for t in range(2)])
        attend([(tile_of(t, d), [(base + held[t], part(d))]) for t in range(2)], diagonal=True)
        take_own_pair(d)
        own_whole(list(range(d + 1)), d)
        prior_keys(list(range(d + 1)), d, True)

    lam_copy(1 - core).wait_recv()
    lam = lamv[head_core, pl.ds(pl.multiple_of(8 * head_no, 8), 8), :][:1, :1]

    def d_copy(t, d):
        where = {"sp": base + held[t], "tp": part(d) * 2 + head_core}
        return remote(dsend.at[t, part(d)], dret.at[chip, head_no], ds_sem.at[t, d],
                      rd_sem.at[chip, head_no], where)

    def d_local(t, d):
        return pltpu.make_async_copy(dsend.at[t, part(d)], dret.at[chip, head_no],
                                     rd_sem.at[chip, head_no])

    def home(t, d):
        return (held[t] == s) & (head_core == core) if d == 0 else False

    @scoped("finish")
    def finish(t, d):
        tile = tile_of(t, d)
        scale = 1.0 / jnp.sum(den[tile], axis=0, keepdims=True)
        out = acc[tile] * scale
        merged = out[:, :chunk] - lam * out[:, chunk:]
        square = jnp.mean(merged * merged, axis=0, keepdims=True)
        normed = (merged * lax.rsqrt(square + HEAD_EPS)).T
        dsend[t, part(d)] = (normed * gain_ref[...] * DIFF_SCALE).astype(BF16)
        if d:
            d_copy(t, d).start()
        else:

            @pl.when(home(t, d))
            def _():
                d_local(t, d).start()

            @pl.when(jnp.logical_not(home(t, d)))
            def _():
                d_copy(t, d).start()

    for d in list(range(1, nchip)) + [0]:
        for t in range(2):
            finish(t, d)

    for d in range(1, nchip):
        for n in range(2):
            with jax.named_scope("w_last"):
                w_side(d, 1 - b, n).wait_recv()
    for h in range(heads):
        for d in range(nchip):
            source = lax.rem(chip + d, nchip)
            piece = dret.at[source, h]
            arrival = remote(piece, piece, ds_sem.at[0, d], rd_sem.at[source, h], pair)
            if d:
                with jax.named_scope("d_wait"):
                    arrival.wait_recv()
            else:

                @pl.when(stays(h))
                def _():
                    pltpu.make_async_copy(dsend.at[0, chip], piece, rd_sem.at[source, h]).wait()

                @pl.when(jnp.logical_not(stays(h)))
                def _():
                    with jax.named_scope("d_wait"):
                        arrival.wait_recv()

    def partial(half, n):
        inner = pl.ds(pl.multiple_of(half * own_rows, own_rows), own_rows)
        total = nn(
            jnp.concatenate([dret[chip, h, inner, :] for h in range(heads)] + [mixed_rows(chip, half)], axis=1),
            wobuf[:, n * cut : (n + 1) * cut])
        for d in range(1, nchip):
            source = lax.rem(chip + d, nchip)
            total = total + nn(
                jnp.concatenate([dret[source, h, inner, :] for h in range(heads)], axis=1),
                wx[d - 1, :, n * cut : (n + 1) * cut])
        return total

    for n in range(npiece):
        mine[n] = partial(1 - core, n).astype(BF16)
        pair_copy(0, n).start()
    for n in range(npiece):
        total = partial(core, n)
        with jax.named_scope("p_wait"):
            pair_copy(0, n).wait_recv()
        total = total + from_pair[n].astype(F32)
        for d in range(1, nchip):
            with jax.named_scope("c_wait"):
                chip_copy(d, n).wait_recv()
            total = total + from_chip[d * npiece + n].astype(F32)
        out_ref[:, n * cut : (n + 1) * cut] = total.astype(BF16)

    with jax.named_scope("s_wait"):
        for copy in copies:
            copy.wait_send()

    for d in range(nchip):
        for h in range(heads):

            @pl.when(jnp.logical_not(stays(h)))
            def _():
                for step in steps(d):
                    q_copy(h, d, step).wait_send()
                    kv_copy(h, d, 0, step).wait_send()

        for dg in range(1, ngroup):

            @pl.when(g + dg < ngroup)
            def _():
                for h in range(heads):
                    for step in steps(d):
                        kv_copy(h, d, dg, step).wait_send()

        for t in range(2):

            @pl.when(needs(t))
            def _():
                fwd(base + held[t], t, 0, d).wait_send()

            if d:
                d_copy(t, d).wait_send()
            else:

                @pl.when(jnp.logical_not(home(t, d)))
                def _():
                    d_copy(t, d).wait_send()

        @pl.loop(0, g)
        def _(back):
            for t in range(2):
                fwd(SQUARE * (g - 1 - back) + held[t], t, 1 + back, d).wait_send()

    for d in range(1, nchip):
        for n in range(2):
            w_cross(d, n).wait_send()
            w_side(d, b, n).wait_send()
    for k in range(1, SQUARE):

        @pl.when(s + k < SQUARE)
        def _():
            st_copy(k).wait_send()

        @pl.loop(0, g)
        def _(back):
            st_pass(back, k).wait_send()

    for dg in range(1, ngroup):

        @pl.when(g + dg < ngroup)
        def _():
            st_later(dg).wait_send()

    for d in range(nchip):
        for n in range(npiece):
            pair_copy(d, n).wait_send()
            if d:
                chip_copy(d, n).wait_send()


VMEM = pl.BlockSpec(memory_space=pltpu.VMEM)
ANY = pl.BlockSpec(memory_space=pl.ANY)
SMEM = pl.BlockSpec(memory_space=pltpu.SMEM)
DMA = pltpu.SemaphoreType.DMA


def params(number):
    return pltpu.CompilerParams(
        collective_id=number, has_side_effects=True, vmem_limit_bytes=VMEM_LIMIT
    )


def on_device(nsp, ntp, tokens, norm_gain, w_query_one, w_query_two, w_key_one, w_key_two, w_value,
              mix_lambda, head_gain, w_ret_query, w_ret_key, w_ret_value, retain_log, init_state,
              w_out_diff, w_out_ret):
    weights = (w_query_one, w_query_two, w_key_one, w_key_two, w_value, w_ret_query, w_ret_key, w_ret_value)
    widths = tuple(w.shape[1] for w in weights)
    own_rows, model = tokens.shape
    rows = own_rows * ntp
    nchip = ntp // 2
    ngroup = nsp // SQUARE
    chunk = rows // nchip
    heads = mix_lambda.shape[0]
    rheads, hd, val = init_state.shape
    kw = widths[2]
    width = w_out_diff.shape[1]
    npiece = 4
    cut = width // npiece
    return pl.pallas_call(
        functools.partial(layer_kernel, nsp, ntp, widths, heads, rheads),
        out_shape=jax.ShapeDtypeStruct((own_rows, width), BF16),
        in_specs=[SMEM] + [VMEM] * 5 + [ANY] * (len(weights) + 2),
        out_specs=VMEM,
        scratch_shapes=[
            pltpu.VMEM((ntp, own_rows, model), BF16),
            pltpu.VMEM((model, sum(widths)), BF16),
            pltpu.VMEM((w_out_diff.shape[0] + w_out_ret.shape[0], width), BF16),
            pltpu.VMEM((nchip - 1, w_out_diff.shape[0], width), BF16),
            pltpu.VMEM((heads, nchip, chunk, kw), BF16),
            pltpu.VMEM((heads, nchip, 2 * chunk, kw), BF16),
            pltpu.VMEM((nsp, nchip, 2 * chunk, kw), BF16),
            pltpu.VMEM((2, nchip, chunk, kw), BF16),
            pltpu.VMEM((2 * nchip, 2 * chunk, kw), BF16),
            pltpu.VMEM((2, 8 * heads, 128), F32),
            pltpu.VMEM((2 * nchip, 8, 2 * chunk), F32),
            pltpu.VMEM((2 * nchip, 8, 2 * chunk), F32),
            pltpu.VMEM((2 * nchip, val, 2 * chunk), F32),
            pltpu.VMEM((2, nchip, chunk, val), BF16),
            pltpu.VMEM((nchip, heads, chunk, val), BF16),
            pltpu.VMEM((nsp, rheads * hd + 16, val), BF16),
            pltpu.VMEM((rows, sum(widths[5:])), BF16),
            pltpu.VMEM((rheads, rows // BLOCK, BLOCK, BLOCK), F32),
            pltpu.VMEM((rheads, rows // BLOCK, BLOCK, 128), F32),
            pltpu.VMEM((rheads, rows, val), F32),
            pltpu.VMEM((rheads, rows // BLOCK, rheads * hd, val), F32),
            pltpu.VMEM((rows, rheads * val), BF16),
            pltpu.VMEM((nchip * npiece, own_rows, cut), BF16),
            pltpu.VMEM((nchip * npiece, own_rows, cut), BF16),
            pltpu.VMEM((nchip * npiece, own_rows, cut), BF16),
            pltpu.VMEM((nchip * npiece, own_rows, cut), BF16),
            DMA((len(weights) + 2,)),
            DMA((2,)),
            DMA((nchip, 2)),
            DMA((nchip, 2)),
            DMA((ntp, 2)),
            DMA((nchip - 1, 2)),
            DMA((nchip - 1, 2)),
            DMA((nchip - 1, 2, 2)),
            DMA((heads, 2 * nchip - 1)),
            DMA((heads, 2 * nchip - 1)),
            DMA((max(ngroup - 1, 1), heads, 2 * nchip - 1)),
            DMA((ngroup, 2, nchip)),
            DMA((2, nchip)),
            DMA((nsp, nchip)),
            DMA((2, nchip)),
            DMA((nchip, heads)),
            DMA((SQUARE,)),
            DMA((ngroup,)),
            DMA((ngroup, SQUARE)),
            DMA((nsp,)),
            DMA((nchip, npiece)),
            DMA((nchip, npiece)),
            DMA((nchip, npiece)),
            DMA((nchip, npiece)),
        ],
        compiler_params=params(0),
        name="layer",
    )(mix_lambda, tokens, norm_gain[None, :], head_gain[None, :], retain_log, init_state, *weights,
      w_out_diff, w_out_ret)


def solution(mesh):
    in_specs = (
        P(("sp", "tp"), None),
        P(),
        P(None, "tp"),
        P(None, "tp"),
        P(None, "tp"),
        P(None, "tp"),
        P(None, "tp"),
        P("tp"),
        P(),
        P(None, "tp"),
        P(None, "tp"),
        P(None, "tp"),
        P("tp", "sp"),
        P("tp", None, None),
        P("tp", None),
        P("tp", None),
    )
    body = functools.partial(on_device, mesh.shape["sp"], mesh.shape["tp"])
    return jax.shard_map(
        body, mesh=mesh, in_specs=in_specs, out_specs=P(("sp", "tp"), None), check_vma=False
    )
```

```python
import functools

import jax
import jax.numpy as jnp
from jax import lax
from jax.experimental import pallas as pl
from jax.experimental.pallas import tpu as pltpu
from jax.sharding import PartitionSpec as P

BLOCK = 256
SQUARE = 4
NORM_EPS = 1e-06
HEAD_EPS = 1e-05
DIFF_SCALE = 0.8
HIGHEST = lax.Precision.HIGHEST
MESH = pl.DeviceIdType.MESH
F32 = jnp.float32
BF16 = jnp.bfloat16
VMEM_LIMIT = 60 * 1024 * 1024


def remote(src, dst, send, recv, where):
    return pltpu.make_async_remote_copy(
        src_ref=src, dst_ref=dst, send_sem=send, recv_sem=recv,
        device_id=where, device_id_type=MESH,
    )


def scoped(name):
    def wrap(step):
        def run(*args, **kw):
            with jax.named_scope(name):
                return step(*args, **kw)
        return run
    return wrap


def head_norm(values):
    return values * lax.rsqrt(jnp.mean(values * values, axis=-1, keepdims=True) + HEAD_EPS)


def nn(a, b, **kw):
    return lax.dot_general(a, b, (((1,), (0,)), ((), ())), preferred_element_type=F32, **kw)


def nt(a, b):
    return lax.dot_general(a, b, (((1,), (1,)), ((), ())), preferred_element_type=F32)


def tn(a, b):
    return lax.dot_general(a, b, (((0,), (0,)), ((), ())), preferred_element_type=F32)


def layer_kernel(nsp, ntp, widths, heads, rheads, lam_ref, tokens_ref, ngain_ref, gain_ref, log_ref,
                 init_ref, *refs):
    nw = len(widths)
    w_refs = refs[:nw]
    wd_ref, wr_ref, out_ref = refs[nw : nw + 3]
    (gat, wbuf, wobuf, wx, sndq, sndkv, kvb, qraw, qs, lamv, peak, den, acc, dsend, dret, sts, rbuf,
     decay, along, rmid, upd, mixr, mine, sent, from_pair, from_chip, kept, outv, wsem, lsem, pair_send, cross_send,
     grecv, wx_send, wx_side, wx_recv, sq_sem, skv_sem, inter_sem, fwd_sem, rq_sem, rkv_sem, ds_sem,
     rd_sem, st_send, st_up, st_on, st_recv, mpair_send, mpair_recv, mchip_send, mchip_recv, osem) = refs[nw + 3 :]
    me = lax.axis_index("sp")
    b = lax.rem(me, 2)
    ngroup = nsp // SQUARE
    g = me // SQUARE
    s = lax.rem(me, SQUARE)
    side = {"sp": me + 1 - 2 * b}
    tme = lax.axis_index("tp")
    core = lax.rem(tme, 2)
    chip = tme // 2
    nchip = ntp // 2
    tpair = tme + 1 - 2 * core
    pair = {"tp": tpair}
    own_rows = tokens_ref.shape[0]
    rows = own_rows * ntp
    chunk = rows // nchip
    kw = widths[2]
    hd = kw // heads
    val = gain_ref.shape[1]

    held = (core, SQUARE - 1 - core)
    others = (1 - core, 2 + core)
    land = lax.rem((s + 1) // 2, 2)
    head_core = s // 2
    head_no = lax.rem(s, 2)
    base = SQUARE * g

    barrier = pltpu.get_barrier_semaphore()

    def greet(where):
        pl.semaphore_signal(barrier, inc=1, device_id=where, device_id_type=MESH)

    for k in range(1, ntp):
        greet({"tp": lax.rem(tme + k, ntp)})
    for k in range(1, SQUARE):
        for n in range(ntp):
            greet({"sp": base + lax.rem(s + k, SQUARE), "tp": n})
    for dg in range(1, ngroup):

        @pl.when(g + dg < ngroup)
        def _():
            for h in range(2):
                greet({"sp": base + SQUARE * dg + 2 * core + h, "tp": chip * 2 + land})
            greet({"sp": me + SQUARE * dg})

        @pl.when(g >= dg)
        def _():
            for t in range(2):
                greet({"sp": base - SQUARE * dg + held[t], "tp": chip * 2 + head_core})
            greet({"sp": me - SQUARE * dg})

    order = (0, 1, 2, 3, 4, 5, 6, 7)
    starts = [sum(widths[:n]) for n in range(nw)]
    loads = {}
    for n in order:
        at = starts[n]
        loads[n] = pltpu.make_async_copy(w_refs[n], wbuf.at[:, at : at + widths[n]], wsem.at[n])
        loads[n].start()
    depth = wd_ref.shape[0]
    out_loads = [
        pltpu.make_async_copy(wd_ref, wobuf.at[:depth], wsem.at[nw]),
        pltpu.make_async_copy(wr_ref, wobuf.at[depth:], wsem.at[nw + 1]),
    ]
    for load in out_loads:
        load.start()
    floats = tokens_ref[...].astype(F32)
    gat[tme] = (
        floats * lax.rsqrt(jnp.mean(floats * floats, axis=-1, keepdims=True) + NORM_EPS) * ngain_ref[...]
    ).astype(BF16)
    for h in range(heads):
        lamv[core, 8 * h : 8 * h + 8, :] = jnp.full((8, 128), lam_ref[h], F32)
    pl.semaphore_wait(barrier, (ntp - 1) + (SQUARE - 1) * ntp + 3 * (ngroup - 1))
    copies = []

    def begin(copy):
        copies.append(copy)
        copy.start()

    def slab(which, half):
        return gat.at[which, pl.ds(half * (own_rows // 2), own_rows // 2)]

    def crossing():
        for d in range(1, nchip):
            there = {"tp": lax.rem(chip + d, nchip) * 2 + core}
            for half in range(2):
                yield remote(slab(tme, half), slab(tme, half), cross_send.at[d, half],
                             grecv.at[tme, half], there)

    def cross(which):
        @pl.when(core == which)
        def _():
            for copy in crossing():
                copy.start()

    cross(0)
    copies.extend(crossing())

    def pair_slab(which, half):
        return remote(slab(which, half), slab(which, half), pair_send.at[which // 2, half],
                      grecv.at[which, half], pair)

    @scoped("landed")
    def landed(which, half):
        remote(slab(which, half), slab(which, half), pair_send.at[which // 2, half],
               grecv.at[which, half], pair).wait_recv()

    def lam_copy(who):
        return remote(lamv.at[who], lamv.at[who], lsem.at[0], lsem.at[1], pair)

    def part(d):
        return lax.rem(chip + nchip - d, nchip)

    def keys_at(d):
        return pl.ds(pl.multiple_of(part(d) * chunk, chunk), chunk)

    def steps(d):
        return ((0, 0, 2),) if d == 0 else ((2 * d - 1, 0, 1), (2 * d, 1, 1))

    def q_rows(ref, at, step):
        return ref.at[at, pl.ds(step[1] * own_rows, step[2] * own_rows)]

    def kv_rows(ref, at, step):
        return ref.at[at, pl.ds(step[1] * 2 * own_rows, step[2] * 2 * own_rows)]

    def q_copy(h, d, step):
        where = {"sp": base + 2 * core + h, "tp": chip * 2 + land}
        return remote(q_rows(sndq.at[h], part(d), step), q_rows(qraw.at[s // 2], part(d), step),
                      sq_sem.at[h, step[0]], rq_sem.at[s // 2, d], where)

    def kv_copy(h, d, dg, step):
        where = {"sp": base + SQUARE * dg + 2 * core + h, "tp": chip * 2 + land}
        sem = skv_sem.at[h, step[0]] if dg == 0 else inter_sem.at[dg - 1, h, step[0]]
        return remote(kv_rows(sndkv.at[h], part(d), step), kv_rows(kvb.at[me], part(d), step), sem,
                      rkv_sem.at[me, d], where)

    def q_local(h, d, step):
        return pltpu.make_async_copy(q_rows(sndq.at[h], part(d), step),
                                     q_rows(qraw.at[s // 2], part(d), step), rq_sem.at[s // 2, d])

    def kv_local(h, d, step):
        return pltpu.make_async_copy(kv_rows(sndkv.at[h], part(d), step),
                                     kv_rows(kvb.at[me], part(d), step), rkv_sem.at[me, d])

    def stays(h):
        return (2 * core + h == s) & (land == core)

    def fwd(span, t, dg, d):
        piece = kvb.at[span, part(d)]
        return remote(piece, piece, fwd_sem.at[dg, t, d], rkv_sem.at[span, d], pair)

    lane = lax.broadcasted_iota(jnp.int32, (chunk, 128), 1)

    @scoped("project")
    def project(d, step):
        number, first, slabs = step
        count = slabs * own_rows
        rows_in = gat[pl.ds(part(d) * 2 + first, slabs)].reshape(count, gat.shape[2])
        low = lane[:count] < hd

        def product(lo, hi):
            if d == 0:
                for n in range(lo, hi):
                    loads[n].wait()
            span = sum(widths[lo:hi])
            return nn(rows_in, wbuf[:, starts[lo] : starts[lo] + span]).astype(BF16).astype(F32)

        def by_head(pairs):
            one, two = pairs[:, :kw], pairs[:, kw:]
            return (jnp.where(low, one, pltpu.roll(two, hd, 1)),
                    jnp.where(low, pltpu.roll(one, kw - hd, 1), two))

        queries = by_head(product(0, 2) * hd ** (-0.5))
        for h in range(heads):
            sndq[h, part(d), first * own_rows : first * own_rows + count] = queries[h].astype(BF16)
        keys = by_head(product(2, 4))
        values = product(4, 5)
        for h in range(heads):
            turned = values[:, h * val : (h + 1) * val].T.astype(BF16)
            for c in range(slabs):
                at = 2 * own_rows * (first + c)
                rows_of = slice(c * own_rows, (c + 1) * own_rows)
                sndkv[h, part(d), at : at + own_rows] = keys[h][rows_of].astype(BF16)
                sndkv[h, part(d), at + own_rows : at + 2 * own_rows] = turned[:, rows_of]
        for h in range(heads):

            @pl.when(stays(h))
            def _():
                q_local(h, d, step).start()
                kv_local(h, d, step).start()

            @pl.when(jnp.logical_not(stays(h)))
            def _():
                q_copy(h, d, step).start()
                kv_copy(h, d, 0, step).start()

    def to_later(d, step, only=None):
        for dg in range(1, ngroup):
            goes = g + dg < ngroup
            if only is not None:
                goes = goes & (core == only)

            @pl.when(goes)
            def _():
                for h in range(heads):
                    kv_copy(h, d, dg, step).start()

    @scoped("project_ret")
    def project_ret(d):
        both = gat[pl.ds(part(d) * 2, 2)].reshape(chunk, gat.shape[2])
        if d == 0:
            for n in range(5, 8):
                loads[n].wait()
        span = sum(widths[5:8])
        for c in range(0, span, 256):
            rbuf[keys_at(d), c : c + 256] = nn(
                both, wbuf[:, starts[5] + c : starts[5] + c + 256]).astype(BF16)

    wpiece = depth // 4

    def w_rows(ref, half, n):
        return ref.at[pl.ds(pl.multiple_of(half * 2 * wpiece, 2 * wpiece) + n * wpiece, wpiece)]

    def w_cross(d, n):
        there = {"tp": lax.rem(chip + d, nchip) * 2 + core}
        return remote(w_rows(wobuf, b, n), w_rows(wx.at[nchip - d - 1], b, n), wx_send.at[d - 1, n],
                      wx_recv.at[nchip - d - 1, b, n], there)

    def w_side(d, half, n):
        piece = w_rows(wx.at[d - 1], half, n)
        return remote(piece, piece, wx_side.at[d - 1, n], wx_recv.at[d - 1, half, n], side)

    @scoped("w_pass")
    def w_pass(n):
        for d in range(1, nchip):
            w_side(d, b, n).wait_recv()
            w_side(d, b, n).start()

    for half in range(2):
        begin(pair_slab(tme, half))
    for d in range(1, nchip):
        for half in range(2):
            copies.append(pair_slab(part(d) * 2 + core, half))
    begin(lam_copy(core))
    peak[...] = jnp.full(peak.shape, -jnp.inf, F32)
    den[...] = jnp.zeros(den.shape, F32)
    acc[...] = jnp.zeros(acc.shape, F32)
    for half in range(2):
        landed(tpair, half)
    project(0, steps(0)[0])
    to_later(0, steps(0)[0], 1)
    cross(1)
    project_ret(0)

    blk = BLOCK
    nblk = rows // blk
    rkw = rheads * hd
    tt = lax.broadcasted_iota(jnp.int32, (blk, blk), 0)
    uu = lax.broadcasted_iota(jnp.int32, (blk, blk), 1)
    rlane = lax.broadcasted_iota(jnp.int32, (blk, rkw), 1)
    srow = lax.broadcasted_iota(jnp.int32, (rkw, val), 0)

    def ours(iota, h):
        return (iota >= h * hd) & (iota < (h + 1) * hd)

    @scoped("decays")
    def decays():
        for h in range(rheads):
            for n in range(nblk):
                row = log_ref[h : h + 1, n * blk : (n + 1) * blk]
                full = jnp.broadcast_to(row, (blk, blk))
                c_col = jnp.sum(jnp.where(uu <= tt, full, 0.0), axis=1, keepdims=True)
                l_col = jnp.sum(jnp.where(uu == tt, full, 0.0), axis=1, keepdims=True)
                c_row = jnp.sum(jnp.where(tt <= uu, l_col, 0.0), axis=0, keepdims=True)
                decay[h, n] = jnp.exp(jnp.where(uu <= tt, c_col - c_row, -jnp.inf))
                along[h, n] = jnp.broadcast_to(c_col, (blk, 128))

    def blocks_of(d):
        for i in range(chunk // blk):
            n = part(d) * (chunk // blk) + i
            yield n, pl.ds(pl.multiple_of(n * blk, blk), blk)

    @scoped("ret_states")
    def ret_states(d):
        for n, at in blocks_of(d):
            keys = rbuf[at, rkw : 2 * rkw].astype(F32) * hd ** (-0.5)
            for h in range(rheads):
                c = along[h, n]
                kd = (keys * jnp.exp(c[blk - 1 : blk, :1] - c[:, :1])).astype(BF16)
                values = rbuf[at, 2 * rkw + h * val : 2 * rkw + (h + 1) * val]
                upd[h, n] = jnp.where(ours(srow, h), tn(kd, values), 0.0)

    @scoped("ret_inner")
    def ret_inner(d):
        for n, at in blocks_of(d):
            keys = rbuf[at, rkw : 2 * rkw]
            for h in range(rheads):
                query = jnp.where(ours(rlane, h), rbuf[at, :rkw].astype(F32), 0.0)
                raw = nt(query.astype(BF16), keys)
                weights = (raw * hd ** (-0.5) * decay[h, n]).astype(BF16)
                rmid[h, at, :] = nn(weights, rbuf[at, 2 * rkw + h * val : 2 * rkw + (h + 1) * val])

    logrow = lax.broadcasted_iota(jnp.int32, (16, val), 0)

    def put_state(slot, state, logs):
        sts[slot, :rkw, :] = state.astype(BF16)
        tile = jnp.zeros((16, val), F32)
        for h in range(rheads):
            wide = jnp.broadcast_to(logs[h], (16, val))
            hi = wide.astype(BF16).astype(F32)
            tile = jnp.where(logrow == 2 * h, hi, tile)
            tile = jnp.where(logrow == 2 * h + 1, wide - hi, tile)
        sts[slot, rkw:, :] = tile.astype(BF16)

    def join(slot, states):
        piece = sts[slot, :rkw, :].astype(F32)
        logs = sts[slot, rkw:, :].astype(F32)
        return tuple(
            jnp.exp(logs[2 * h : 2 * h + 1] + logs[2 * h + 1 : 2 * h + 2]) * states[h]
            + jnp.where(ours(srow, h), piece, 0.0)
            for h in range(rheads)
        )

    def st_copy(k):
        return remote(sts.at[me], sts.at[me], st_send.at[k], st_recv.at[me],
                      {"sp": base + lax.rem(s + k, SQUARE)})

    def st_later(dg):
        return remote(sts.at[me], sts.at[me], st_up.at[dg], st_recv.at[me], {"sp": me + SQUARE * dg})

    def st_pass(back, k):
        span = me - SQUARE * (back + 1)
        return remote(sts.at[span], sts.at[span], st_on.at[back, k], st_recv.at[span],
                      {"sp": base + lax.rem(s + k, SQUARE)})

    def st_wait(span):
        remote(sts.at[span], sts.at[span], st_send.at[0], st_recv.at[span], pair).wait_recv()

    @scoped("span_state")
    def span_state():
        total = jnp.zeros((rkw, val), F32)
        logs = []
        for h in range(rheads):
            state = jnp.zeros((rkw, val), F32)
            log_all = jnp.zeros((1, 1), F32)
            for n in range(nblk):
                last = along[h, n, blk - 1 : blk, :1]
                state = jnp.exp(last) * state + upd[h, n]
                log_all = log_all + last
            total = total + state
            logs.append(log_all)
        put_state(me, total, logs)
        for k in range(1, SQUARE):

            @pl.when(s + k < SQUARE)
            def _():
                st_copy(k).start()

        for dg in range(1, ngroup):

            @pl.when(g + dg < ngroup)
            def _():
                st_later(dg).start()

    @scoped("pass_states")
    def pass_states():
        @pl.loop(0, g)
        def _(back):
            st_wait(me - SQUARE * (back + 1))
            for k in range(1, SQUARE):
                st_pass(back, k).start()

    @scoped("ret_finish")
    def ret_finish():
        first = []
        for h in range(rheads):
            parts = ([jnp.zeros((hd, val), F32)] * h + [init_ref[h]]
                     + [jnp.zeros((hd, val), F32)] * (rheads - 1 - h))
            first.append(jnp.concatenate(parts, axis=0) if rheads > 1 else parts[0])

        @pl.loop(0, g)
        def _(back):
            for k in range(1, SQUARE):
                st_wait(base - SQUARE * (back + 1) + lax.rem(s + k, SQUARE))

        @pl.loop(0, s)
        def _(slot):
            st_wait(base + slot)

        carried = lax.fori_loop(0, me, join, tuple(first))
        for h in range(rheads):
            state = carried[h]
            for n in range(nblk):
                at = slice(n * blk, (n + 1) * blk)
                c = along[h, n]
                query = rbuf[at, :rkw].astype(F32) * jnp.exp(c[:, :1])
                result = rmid[h, at, :] + nn(query, state, precision=HIGHEST)
                if n + 1 < nblk:
                    state = jnp.exp(c[blk - 1 : blk, :1]) * state + upd[h, n]
                mixr[at, h * val : (h + 1) * val] = head_norm(result).astype(BF16)

    decays()
    ret_states(0)
    ret_inner(0)
    to_later(0, steps(0)[0], 0)

    @scoped("take")
    def take(span, t, d, local):
        if local:
            here = (held[t] == s) & (head_core == core)

            @pl.when(here)
            def _():
                pltpu.make_async_copy(sndq.at[0, part(d)], qraw.at[t, part(d)], rq_sem.at[t, d]).wait()
                pltpu.make_async_copy(sndkv.at[0, part(d)], kvb.at[span, part(d)],
                                      rkv_sem.at[span, d]).wait()

            @pl.when(jnp.logical_not(here))
            def _():
                remote(qraw.at[t, part(d)], qraw.at[t, part(d)], sq_sem.at[0, d],
                       rq_sem.at[t, d], pair).wait_recv()
                remote(kvb.at[span, part(d)], kvb.at[span, part(d)], skv_sem.at[0, d],
                       rkv_sem.at[span, d], pair).wait_recv()
        else:
            remote(kvb.at[span, part(d)], kvb.at[span, part(d)], skv_sem.at[0, d],
                   rkv_sem.at[span, d], pair).wait_recv()

    def ready(t, d):
        tile = t * nchip + part(d)
        value = qraw[t, part(d)].astype(F32)
        qs[tile, :chunk] = jnp.where(lane < hd, value, 0.0).astype(BF16)
        qs[tile, chunk:] = jnp.where(lane < hd, 0.0, value).astype(BF16)

    def needs(t):
        return (core == 1) | (t == 0)

    def take_own(d):
        for t in range(2):
            take(base + held[t], t, d, True)

            @pl.when(needs(t))
            def _():
                fwd(base + held[t], t, 0, d).start()

        for t in range(2):
            ready(t, d)

    @scoped("take_own_pair")
    def take_own_pair(d):
        for t in range(2):

            @pl.when((core == 0) | (t == 0))
            def _():
                fwd(base + others[t], t, 0, d).wait_recv()

    krow = lax.broadcasted_iota(jnp.int32, (chunk, 2 * chunk), 0)
    qcol = lax.rem(lax.broadcasted_iota(jnp.int32, (chunk, 2 * chunk), 1), chunk)

    @scoped("attend")
    def attend(items, diagonal=False):
        scores = []
        for tile, blocks in items:
            row = []
            for span, a in blocks:
                keys = jnp.concatenate(
                    [kvb[span, a, 2 * c * own_rows : (2 * c + 1) * own_rows] for c in range(2)], axis=0)
                raw = nt(keys, qs[tile])
                row.append(jnp.where(krow <= qcol, raw, -jnp.inf) if diagonal else raw)
            scores.append(row)
        for (tile, blocks), row in zip(items, scores):
            old = peak[tile]
            top = old
            for raw in row:
                top = jnp.maximum(top, jnp.max(raw, axis=0, keepdims=True))
            rescale = jnp.exp(old - top)
            total = None
            weighted = None
            for (span, a), raw in zip(blocks, row):
                e = jnp.exp(raw - top[:1])
                sums = jnp.sum(e.reshape(chunk // 8, 8, 2 * chunk), axis=0)
                turned = jnp.concatenate(
                    [kvb[span, a, (2 * c + 1) * own_rows : (2 * c + 2) * own_rows] for c in range(2)],
                    axis=1)
                got = nn(turned, e.astype(BF16))
                total = sums if total is None else total + sums
                weighted = got if weighted is None else weighted + got
            peak[tile] = top
            den[tile] = den[tile] * rescale + total
            acc[tile] = acc[tile] * rescale[:1] + weighted

    def tile_of(t, d):
        return t * nchip + part(d)

    def prior_keys(queries_d, keys_d, fresh):
        @pl.loop(0, g)
        def _(back):
            first = SQUARE * (g - 1 - back)
            for group in range(2):
                slots = held if group == 0 else others
                spans = [first + slots[t] for t in range(2)]
                if fresh:
                    for t in range(2):
                        if group == 0:
                            take(spans[t], t, keys_d, False)
                            fwd(spans[t], t, 1 + back, keys_d).start()
                        else:
                            take(spans[t], t, keys_d, False)
                for e in queries_d:
                    attend([(tile_of(t, e), [(span, part(keys_d)) for span in spans]) for t in range(2)])

    def own_whole(queries_d, keys_d):
        third_t, third_slot = 1 - core, 2 * (1 - core)
        at = part(keys_d)
        attend([item for e in queries_d for item in (
            (nchip + part(e), ((base, at), (base + 1, at))),
            (third_t * nchip + part(e), ((base + third_slot, at),)),
        )])

    width = out_ref.shape[1]
    cut = mine.shape[2]
    npiece = width // cut

    def mixed_rows(which):
        return mixr[pl.ds(pl.multiple_of(which * chunk, chunk), chunk), :]

    def split(d, n, full):
        first, second = full[:own_rows], full[own_rows:]
        mine[d * npiece + n] = jnp.where(core == 0, second, first).astype(BF16)
        kept[d * npiece + n] = jnp.where(core == 0, first, second)
        pair_copy(d, n).start()

    def pair_copy(d, n):
        return remote(mine.at[d * npiece + n], from_pair.at[d * npiece + n], mpair_send.at[d, n],
                      mpair_recv.at[d, n], pair)

    def chip_copy(d, n):
        there = lax.rem(chip + d, nchip) * 2 + core
        return remote(sent.at[d * npiece + n], from_chip.at[d * npiece + n], mchip_send.at[d, n],
                      mchip_recv.at[d, n], {"tp": there})

    @scoped("ret_reduce")
    def ret_reduce():
        out_loads[1].wait()
        for d in range(1, nchip):
            which = lax.rem(chip + d, nchip)
            for n in range(npiece):
                split(d, n, nn(mixed_rows(which), wobuf[depth:, n * cut : (n + 1) * cut]))

    @scoped("ret_send")
    def ret_send():
        for d in range(1, nchip):
            for n in range(npiece):
                pair_copy(d, n).wait_recv()
                at = d * npiece + n
                sent[at] = (kept[at] + from_pair[at].astype(F32)).astype(BF16)
                if n < npiece - 1:
                    chip_copy(d, n).start()

    def slab_in(d, which):
        index = part(d) * 2 + which
        for half in range(2):
            landed(index, half)

            @pl.when(core == which)
            def _():
                pair_slab(index, half).start()

    for d in range(1, nchip):
        slab_in(d, 0)
        project(d, steps(d)[0])

    for d in range(1, nchip):
        slab_in(d, 1)
        if d == nchip - 1:
            out_loads[0].wait()
            for e in range(1, nchip):
                for n in range(2):
                    w_cross(e, n).start()
        project_ret(d)
        ret_states(d)
        if d == nchip - 1:
            span_state()
        project(d, steps(d)[1])
        if d < nchip - 1:
            for step in steps(d):
                to_later(d, step, 1)
        ret_inner(d)
    take_own(0)
    attend([(tile_of(t, 0), [(base + held[t], part(0))]) for t in range(2)], diagonal=True)
    take_own_pair(0)
    own_whole([0], 0)
    pass_states()
    for d in range(1, nchip):
        for step in steps(d):
            to_later(d, step, 0)
    prior_keys([0], 0, True)

    lam_copy(1 - core).wait_recv()
    lam = lamv[head_core, pl.ds(pl.multiple_of(8 * head_no, 8), 8), :][:1, :1]

    def d_copy(t, d):
        where = {"sp": base + held[t], "tp": part(d) * 2 + head_core}
        return remote(dsend.at[t, part(d)], dret.at[chip, head_no], ds_sem.at[t, d],
                      rd_sem.at[chip, head_no], where)

    def d_local(t, d):
        return pltpu.make_async_copy(dsend.at[t, part(d)], dret.at[chip, head_no],
                                     rd_sem.at[chip, head_no])

    def home(t, d):
        return (held[t] == s) & (head_core == core) if d == 0 else False

    @scoped("finish")
    def finish(t, d):
        tile = tile_of(t, d)
        scale = 1.0 / jnp.sum(den[tile], axis=0, keepdims=True)
        out = acc[tile] * scale
        merged = out[:, :chunk] - lam * out[:, chunk:]
        square = jnp.mean(merged * merged, axis=0, keepdims=True)
        normed = (merged * lax.rsqrt(square + HEAD_EPS)).T
        dsend[t, part(d)] = (normed * gain_ref[...] * DIFF_SCALE).astype(BF16)
        if d:
            d_copy(t, d).start()
        else:

            @pl.when(home(t, d))
            def _():
                d_local(t, d).start()

            @pl.when(jnp.logical_not(home(t, d)))
            def _():
                d_copy(t, d).start()

    for d in range(1, nchip):
        take_own(d)
        if d == nchip - 1:
            w_pass(0)
            ret_finish()
            ret_reduce()
            w_pass(1)
            ret_send()
            for step in steps(d):
                to_later(d, step, 1)
        for e in range(d):
            prior_keys([d], e, False)
            own_whole([d], e)
            high = jnp.maximum(part(d), part(e))
            low = jnp.minimum(part(d), part(e))
            attend([(t * nchip + high, [(base + held[t], low)]) for t in range(2)])
        attend([(tile_of(t, d), [(base + held[t], part(d))]) for t in range(2)], diagonal=True)
        take_own_pair(d)
        own_whole(list(range(d + 1)), d)
        if d < nchip - 1:
            prior_keys(list(range(d + 1)), d, True)

    last = nchip - 1
    prior_keys(list(range(1, nchip)), last, True)
    for d in range(1, nchip):
        for t in range(2):
            finish(t, d)
    for d in range(1, nchip):
        chip_copy(d, npiece - 1).start()
    prior_keys([0], last, False)
    for t in range(2):
        finish(t, 0)


    for d in range(1, nchip):
        for n in range(2):
            with jax.named_scope("w_last"):
                w_side(d, 1 - b, n).wait_recv()
    for h in range(heads):
        for d in range(nchip):
            source = lax.rem(chip + d, nchip)
            piece = dret.at[source, h]
            arrival = remote(piece, piece, ds_sem.at[0, d], rd_sem.at[source, h], pair)
            if d:
                with jax.named_scope("d_wait"):
                    arrival.wait_recv()
            else:

                @pl.when(stays(h))
                def _():
                    pltpu.make_async_copy(dsend.at[0, chip], piece, rd_sem.at[source, h]).wait()

                @pl.when(jnp.logical_not(stays(h)))
                def _():
                    with jax.named_scope("d_wait"):
                        arrival.wait_recv()

    def partial(n):
        total = nn(
            jnp.concatenate([dret[chip, h] for h in range(heads)] + [mixed_rows(chip)], axis=1),
            wobuf[:, n * cut : (n + 1) * cut])
        for d in range(1, nchip):
            source = lax.rem(chip + d, nchip)
            total = total + nn(
                jnp.concatenate([dret[source, h] for h in range(heads)], axis=1),
                wx[d - 1, :, n * cut : (n + 1) * cut])
        return total

    def put(n):
        return pltpu.make_async_copy(outv.at[n], out_ref.at[:, n * cut : (n + 1) * cut], osem.at[n])

    for n in range(npiece):
        split(0, n, partial(n))
    for n in range(npiece):
        with jax.named_scope("p_wait"):
            pair_copy(0, n).wait_recv()
        total = kept[n] + from_pair[n].astype(F32)
        for d in range(1, nchip):
            with jax.named_scope("c_wait"):
                chip_copy(d, n).wait_recv()
            total = total + from_chip[d * npiece + n].astype(F32)
        outv[n] = total.astype(BF16)
        put(n).start()

    with jax.named_scope("s_wait"):
        for copy in copies:
            copy.wait_send()

    for d in range(nchip):
        for h in range(heads):

            @pl.when(jnp.logical_not(stays(h)))
            def _():
                for step in steps(d):
                    q_copy(h, d, step).wait_send()
                    kv_copy(h, d, 0, step).wait_send()

        for dg in range(1, ngroup):

            @pl.when(g + dg < ngroup)
            def _():
                for h in range(heads):
                    for step in steps(d):
                        kv_copy(h, d, dg, step).wait_send()

        for t in range(2):

            @pl.when(needs(t))
            def _():
                fwd(base + held[t], t, 0, d).wait_send()

            if d:
                d_copy(t, d).wait_send()
            else:

                @pl.when(jnp.logical_not(home(t, d)))
                def _():
                    d_copy(t, d).wait_send()

        @pl.loop(0, g)
        def _(back):
            for t in range(2):
                fwd(SQUARE * (g - 1 - back) + held[t], t, 1 + back, d).wait_send()

    for d in range(1, nchip):
        for n in range(2):
            w_cross(d, n).wait_send()
            w_side(d, b, n).wait_send()
    for k in range(1, SQUARE):

        @pl.when(s + k < SQUARE)
        def _():
            st_copy(k).wait_send()

        @pl.loop(0, g)
        def _(back):
            st_pass(back, k).wait_send()

    for dg in range(1, ngroup):

        @pl.when(g + dg < ngroup)
        def _():
            st_later(dg).wait_send()

    for d in range(nchip):
        for n in range(npiece):
            pair_copy(d, n).wait_send()
            if d:
                chip_copy(d, n).wait_send()
    for n in range(npiece):
        put(n).wait()


VMEM = pl.BlockSpec(memory_space=pltpu.VMEM)
ANY = pl.BlockSpec(memory_space=pl.ANY)
SMEM = pl.BlockSpec(memory_space=pltpu.SMEM)
DMA = pltpu.SemaphoreType.DMA


def params(number):
    return pltpu.CompilerParams(
        collective_id=number, has_side_effects=True, vmem_limit_bytes=VMEM_LIMIT
    )


def on_device(nsp, ntp, tokens, norm_gain, w_query_one, w_query_two, w_key_one, w_key_two, w_value,
              mix_lambda, head_gain, w_ret_query, w_ret_key, w_ret_value, retain_log, init_state,
              w_out_diff, w_out_ret):
    weights = (w_query_one, w_query_two, w_key_one, w_key_two, w_value, w_ret_query, w_ret_key, w_ret_value)
    widths = tuple(w.shape[1] for w in weights)
    own_rows, model = tokens.shape
    rows = own_rows * ntp
    nchip = ntp // 2
    ngroup = nsp // SQUARE
    chunk = rows // nchip
    heads = mix_lambda.shape[0]
    rheads, hd, val = init_state.shape
    kw = widths[2]
    width = w_out_diff.shape[1]
    npiece = 4
    cut = width // npiece
    return pl.pallas_call(
        functools.partial(layer_kernel, nsp, ntp, widths, heads, rheads),
        out_shape=jax.ShapeDtypeStruct((own_rows, width), BF16),
        in_specs=[SMEM] + [VMEM] * 5 + [ANY] * (len(weights) + 2),
        out_specs=ANY,
        scratch_shapes=[
            pltpu.VMEM((ntp, own_rows, model), BF16),
            pltpu.VMEM((model, sum(widths)), BF16),
            pltpu.VMEM((w_out_diff.shape[0] + w_out_ret.shape[0], width), BF16),
            pltpu.VMEM((nchip - 1, w_out_diff.shape[0], width), BF16),
            pltpu.VMEM((heads, nchip, chunk, kw), BF16),
            pltpu.VMEM((heads, nchip, 2 * chunk, kw), BF16),
            pltpu.VMEM((nsp, nchip, 2 * chunk, kw), BF16),
            pltpu.VMEM((2, nchip, chunk, kw), BF16),
            pltpu.VMEM((2 * nchip, 2 * chunk, kw), BF16),
            pltpu.VMEM((2, 8 * heads, 128), F32),
            pltpu.VMEM((2 * nchip, 8, 2 * chunk), F32),
            pltpu.VMEM((2 * nchip, 8, 2 * chunk), F32),
            pltpu.VMEM((2 * nchip, val, 2 * chunk), F32),
            pltpu.VMEM((2, nchip, chunk, val), BF16),
            pltpu.VMEM((nchip, heads, chunk, val), BF16),
            pltpu.VMEM((nsp, rheads * hd + 16, val), BF16),
            pltpu.VMEM((rows, sum(widths[5:])), BF16),
            pltpu.VMEM((rheads, rows // BLOCK, BLOCK, BLOCK), F32),
            pltpu.VMEM((rheads, rows // BLOCK, BLOCK, 128), F32),
            pltpu.VMEM((rheads, rows, val), F32),
            pltpu.VMEM((rheads, rows // BLOCK, rheads * hd, val), F32),
            pltpu.VMEM((rows, rheads * val), BF16),
            pltpu.VMEM((nchip * npiece, own_rows, cut), BF16),
            pltpu.VMEM((nchip * npiece, own_rows, cut), BF16),
            pltpu.VMEM((nchip * npiece, own_rows, cut), BF16),
            pltpu.VMEM((nchip * npiece, own_rows, cut), BF16),
            pltpu.VMEM((nchip * npiece, own_rows, cut), F32),
            pltpu.VMEM((npiece, own_rows, cut), BF16),
            DMA((len(weights) + 2,)),
            DMA((2,)),
            DMA((nchip, 2)),
            DMA((nchip, 2)),
            DMA((ntp, 2)),
            DMA((nchip - 1, 2)),
            DMA((nchip - 1, 2)),
            DMA((nchip - 1, 2, 2)),
            DMA((heads, 2 * nchip - 1)),
            DMA((heads, 2 * nchip - 1)),
            DMA((max(ngroup - 1, 1), heads, 2 * nchip - 1)),
            DMA((ngroup, 2, nchip)),
            DMA((2, nchip)),
            DMA((nsp, nchip)),
            DMA((2, nchip)),
            DMA((nchip, heads)),
            DMA((SQUARE,)),
            DMA((ngroup,)),
            DMA((ngroup, SQUARE)),
            DMA((nsp,)),
            DMA((nchip, npiece)),
            DMA((nchip, npiece)),
            DMA((nchip, npiece)),
            DMA((nchip, npiece)),
            DMA((npiece,)),
        ],
        compiler_params=params(0),
        name="layer",
    )(mix_lambda, tokens, norm_gain[None, :], head_gain[None, :], retain_log, init_state, *weights,
      w_out_diff, w_out_ret)


def solution(mesh):
    in_specs = (
        P(("sp", "tp"), None),
        P(),
        P(None, "tp"),
        P(None, "tp"),
        P(None, "tp"),
        P(None, "tp"),
        P(None, "tp"),
        P("tp"),
        P(),
        P(None, "tp"),
        P(None, "tp"),
        P(None, "tp"),
        P("tp", "sp"),
        P("tp", None, None),
        P("tp", None),
        P("tp", None),
    )
    body = functools.partial(on_device, mesh.shape["sp"], mesh.shape["tp"])
    return jax.shard_map(
        body, mesh=mesh, in_specs=in_specs, out_specs=P(("sp", "tp"), None), check_vma=False
    )
```

```python
import functools

import jax
import jax.numpy as jnp
from jax import lax
from jax.experimental import pallas as pl
from jax.experimental.pallas import tpu as pltpu
from jax.sharding import PartitionSpec as P

BLOCK = 256
SQUARE = 4
NORM_EPS = 1e-06
HEAD_EPS = 1e-05
DIFF_SCALE = 0.8
HIGHEST = lax.Precision.HIGHEST
MESH = pl.DeviceIdType.MESH
F32 = jnp.float32
BF16 = jnp.bfloat16
VMEM_LIMIT = 60 * 1024 * 1024


def remote(src, dst, send, recv, where):
    return pltpu.make_async_remote_copy(
        src_ref=src, dst_ref=dst, send_sem=send, recv_sem=recv,
        device_id=where, device_id_type=MESH,
    )


def scoped(name):
    def wrap(step):
        def run(*args, **kw):
            with jax.named_scope(name):
                return step(*args, **kw)
        return run
    return wrap


def head_norm(values):
    return values * lax.rsqrt(jnp.mean(values * values, axis=-1, keepdims=True) + HEAD_EPS)


def nn(a, b, **kw):
    return lax.dot_general(a, b, (((1,), (0,)), ((), ())), preferred_element_type=F32, **kw)


def nt(a, b):
    return lax.dot_general(a, b, (((1,), (1,)), ((), ())), preferred_element_type=F32)


def tn(a, b):
    return lax.dot_general(a, b, (((0,), (0,)), ((), ())), preferred_element_type=F32)


def layer_kernel(nsp, ntp, widths, heads, rheads, lam_ref, tokens_ref, ngain_ref, gain_ref, log_ref,
                 init_ref, *refs):
    nw = len(widths)
    w_refs = refs[:nw]
    wd_ref, wr_ref, out_ref = refs[nw : nw + 3]
    (gat, wbuf, wobuf, wx, sndq, sndkv, kvb, qraw, qs, lamv, peak, den, acc, dsend, dret, sts, rbuf,
     decay, along, rmid, upd, mixr, mine, sent, from_pair, from_chip, kept, outv, wsem, lsem, pair_send, cross_send,
     grecv, wx_send, wx_side, wx_recv, sq_sem, skv_sem, inter_sem, fwd_sem, rq_sem, rkv_sem, ds_sem,
     rd_sem, st_send, st_up, st_on, st_recv, mpair_send, mpair_recv, mchip_send, mchip_recv, osem) = refs[nw + 3 :]
    me = lax.axis_index("sp")
    b = lax.rem(me, 2)
    ngroup = nsp // SQUARE
    g = me // SQUARE
    s = lax.rem(me, SQUARE)
    side = {"sp": me + 1 - 2 * b}
    tme = lax.axis_index("tp")
    core = lax.rem(tme, 2)
    chip = tme // 2
    nchip = ntp // 2
    tpair = tme + 1 - 2 * core
    pair = {"tp": tpair}
    own_rows = tokens_ref.shape[0]
    rows = own_rows * ntp
    chunk = rows // nchip
    kw = widths[2]
    hd = kw // heads
    val = gain_ref.shape[1]

    held = (core, SQUARE - 1 - core)
    others = (1 - core, 2 + core)
    land = lax.rem((s + 1) // 2, 2)
    head_core = s // 2
    head_no = lax.rem(s, 2)
    base = SQUARE * g

    barrier = pltpu.get_barrier_semaphore()

    def greet(where):
        pl.semaphore_signal(barrier, inc=1, device_id=where, device_id_type=MESH)

    for k in range(1, ntp):
        greet({"tp": lax.rem(tme + k, ntp)})
    for k in range(1, SQUARE):
        for n in range(ntp):
            greet({"sp": base + lax.rem(s + k, SQUARE), "tp": n})
    for dg in range(1, ngroup):

        @pl.when(g + dg < ngroup)
        def _():
            for h in range(2):
                greet({"sp": base + SQUARE * dg + 2 * core + h, "tp": chip * 2 + land})
            greet({"sp": me + SQUARE * dg})

        @pl.when(g >= dg)
        def _():
            for t in range(2):
                greet({"sp": base - SQUARE * dg + held[t], "tp": chip * 2 + head_core})
            greet({"sp": me - SQUARE * dg})

    order = (0, 1, 2, 3, 4, 5, 6, 7)
    starts = [sum(widths[:n]) for n in range(nw)]
    loads = {}
    for n in order:
        at = starts[n]
        loads[n] = pltpu.make_async_copy(w_refs[n], wbuf.at[:, at : at + widths[n]], wsem.at[n])
        loads[n].start()
    depth = wd_ref.shape[0]
    out_loads = [
        pltpu.make_async_copy(wd_ref, wobuf.at[:depth], wsem.at[nw]),
        pltpu.make_async_copy(wr_ref, wobuf.at[depth:], wsem.at[nw + 1]),
    ]
    for load in out_loads:
        load.start()
    floats = tokens_ref[...].astype(F32)
    gat[tme] = (
        floats * lax.rsqrt(jnp.mean(floats * floats, axis=-1, keepdims=True) + NORM_EPS) * ngain_ref[...]
    ).astype(BF16)
    for h in range(heads):
        lamv[core, 8 * h : 8 * h + 8, :] = jnp.full((8, 128), lam_ref[h], F32)
    pl.semaphore_wait(barrier, (ntp - 1) + (SQUARE - 1) * ntp + 3 * (ngroup - 1))
    copies = []

    def begin(copy):
        copies.append(copy)
        copy.start()

    def slab(which, half):
        return gat.at[which, pl.ds(half * (own_rows // 2), own_rows // 2)]

    def crossing():
        for d in range(1, nchip):
            there = {"tp": lax.rem(chip + d, nchip) * 2 + core}
            for half in range(2):
                yield remote(slab(tme, half), slab(tme, half), cross_send.at[d, half],
                             grecv.at[tme, half], there)

    def cross(which):
        @pl.when(core == which)
        def _():
            for copy in crossing():
                copy.start()

    cross(0)
    copies.extend(crossing())

    def pair_slab(which, half):
        return remote(slab(which, half), slab(which, half), pair_send.at[which // 2, half],
                      grecv.at[which, half], pair)

    @scoped("landed")
    def landed(which, half):
        remote(slab(which, half), slab(which, half), pair_send.at[which // 2, half],
               grecv.at[which, half], pair).wait_recv()

    def lam_copy(who):
        return remote(lamv.at[who], lamv.at[who], lsem.at[0], lsem.at[1], pair)

    def part(d):
        return lax.rem(chip + nchip - d, nchip)

    def keys_at(d):
        return pl.ds(pl.multiple_of(part(d) * chunk, chunk), chunk)

    def steps(d):
        return ((0, 0, 2),) if d == 0 else ((2 * d - 1, 0, 1), (2 * d, 1, 1))

    def q_rows(ref, at, step):
        return ref.at[at, pl.ds(step[1] * own_rows, step[2] * own_rows)]

    def kv_rows(ref, at, step):
        return ref.at[at, pl.ds(step[1] * 2 * own_rows, step[2] * 2 * own_rows)]

    def q_copy(h, d, step):
        where = {"sp": base + 2 * core + h, "tp": chip * 2 + land}
        return remote(q_rows(sndq.at[h], part(d), step), q_rows(qraw.at[s // 2], part(d), step),
                      sq_sem.at[h, step[0]], rq_sem.at[s // 2, d], where)

    def kv_copy(h, d, dg, step):
        where = {"sp": base + SQUARE * dg + 2 * core + h, "tp": chip * 2 + land}
        sem = skv_sem.at[h, step[0]] if dg == 0 else inter_sem.at[dg - 1, h, step[0]]
        return remote(kv_rows(sndkv.at[h], part(d), step), kv_rows(kvb.at[me], part(d), step), sem,
                      rkv_sem.at[me, d], where)

    def q_local(h, d, step):
        return pltpu.make_async_copy(q_rows(sndq.at[h], part(d), step),
                                     q_rows(qraw.at[s // 2], part(d), step), rq_sem.at[s // 2, d])

    def kv_local(h, d, step):
        return pltpu.make_async_copy(kv_rows(sndkv.at[h], part(d), step),
                                     kv_rows(kvb.at[me], part(d), step), rkv_sem.at[me, d])

    def stays(h):
        return (2 * core + h == s) & (land == core)

    def fwd(span, t, dg, d):
        piece = kvb.at[span, part(d)]
        return remote(piece, piece, fwd_sem.at[dg, t, d], rkv_sem.at[span, d], pair)

    lane = lax.broadcasted_iota(jnp.int32, (chunk, 128), 1)

    @scoped("project")
    def project(d, step):
        number, first, slabs = step
        count = slabs * own_rows
        rows_in = gat[pl.ds(part(d) * 2 + first, slabs)].reshape(count, gat.shape[2])
        low = lane[:count] < hd

        def product(lo, hi):
            if d == 0:
                for n in range(lo, hi):
                    loads[n].wait()
            span = sum(widths[lo:hi])
            return nn(rows_in, wbuf[:, starts[lo] : starts[lo] + span]).astype(BF16).astype(F32)

        def by_head(pairs):
            one, two = pairs[:, :kw], pairs[:, kw:]
            return (jnp.where(low, one, pltpu.roll(two, hd, 1)),
                    jnp.where(low, pltpu.roll(one, kw - hd, 1), two))

        queries = by_head(product(0, 2) * hd ** (-0.5))
        for h in range(heads):
            sndq[h, part(d), first * own_rows : first * own_rows + count] = queries[h].astype(BF16)
        keys = by_head(product(2, 4))
        values = product(4, 5)
        for h in range(heads):
            turned = values[:, h * val : (h + 1) * val].T.astype(BF16)
            for c in range(slabs):
                at = 2 * own_rows * (first + c)
                rows_of = slice(c * own_rows, (c + 1) * own_rows)
                sndkv[h, part(d), at : at + own_rows] = keys[h][rows_of].astype(BF16)
                sndkv[h, part(d), at + own_rows : at + 2 * own_rows] = turned[:, rows_of]
        for h in range(heads):

            @pl.when(stays(h))
            def _():
                q_local(h, d, step).start()
                kv_local(h, d, step).start()

            @pl.when(jnp.logical_not(stays(h)))
            def _():
                q_copy(h, d, step).start()
                kv_copy(h, d, 0, step).start()

    def to_later(d, step, only=None):
        for dg in range(1, ngroup):
            goes = g + dg < ngroup
            if only is not None:
                goes = goes & (core == only)

            @pl.when(goes)
            def _():
                for h in range(heads):
                    kv_copy(h, d, dg, step).start()

    @scoped("project_ret")
    def project_ret(d):
        both = gat[pl.ds(part(d) * 2, 2)].reshape(chunk, gat.shape[2])
        if d == 0:
            for n in range(5, 8):
                loads[n].wait()
        span = sum(widths[5:8])
        for c in range(0, span, 256):
            rbuf[keys_at(d), c : c + 256] = nn(
                both, wbuf[:, starts[5] + c : starts[5] + c + 256]).astype(BF16)

    wpiece = depth // 4

    def w_rows(ref, half, n):
        return ref.at[pl.ds(pl.multiple_of(half * 2 * wpiece, 2 * wpiece) + n * wpiece, wpiece)]

    def w_cross(d, n):
        there = {"tp": lax.rem(chip + d, nchip) * 2 + core}
        return remote(w_rows(wobuf, b, n), w_rows(wx.at[nchip - d - 1], b, n), wx_send.at[d - 1, n],
                      wx_recv.at[nchip - d - 1, b, n], there)

    def w_side(d, half, n):
        piece = w_rows(wx.at[d - 1], half, n)
        return remote(piece, piece, wx_side.at[d - 1, n], wx_recv.at[d - 1, half, n], side)

    @scoped("w_pass")
    def w_pass(n):
        for d in range(1, nchip):
            w_side(d, b, n).wait_recv()
            w_side(d, b, n).start()

    for half in range(2):
        begin(pair_slab(tme, half))
    for d in range(1, nchip):
        for half in range(2):
            copies.append(pair_slab(part(d) * 2 + core, half))
    begin(lam_copy(core))
    peak[...] = jnp.full(peak.shape, -jnp.inf, F32)
    den[...] = jnp.zeros(den.shape, F32)
    acc[...] = jnp.zeros(acc.shape, F32)
    for half in range(2):
        landed(tpair, half)
    project(0, steps(0)[0])
    to_later(0, steps(0)[0], 1)
    cross(1)
    project_ret(0)

    blk = BLOCK
    nblk = rows // blk
    rkw = rheads * hd
    tt = lax.broadcasted_iota(jnp.int32, (blk, blk), 0)
    uu = lax.broadcasted_iota(jnp.int32, (blk, blk), 1)
    rlane = lax.broadcasted_iota(jnp.int32, (blk, rkw), 1)
    srow = lax.broadcasted_iota(jnp.int32, (rkw, val), 0)

    def ours(iota, h):
        return (iota >= h * hd) & (iota < (h + 1) * hd)

    @scoped("decays")
    def decays():
        for h in range(rheads):
            for n in range(nblk):
                row = log_ref[h : h + 1, n * blk : (n + 1) * blk]
                full = jnp.broadcast_to(row, (blk, blk))
                c_col = jnp.sum(jnp.where(uu <= tt, full, 0.0), axis=1, keepdims=True)
                l_col = jnp.sum(jnp.where(uu == tt, full, 0.0), axis=1, keepdims=True)
                c_row = jnp.sum(jnp.where(tt <= uu, l_col, 0.0), axis=0, keepdims=True)
                decay[h, n] = jnp.exp(jnp.where(uu <= tt, c_col - c_row, -jnp.inf))
                along[h, n] = jnp.broadcast_to(c_col, (blk, 128))

    def blocks_of(d):
        for i in range(chunk // blk):
            n = part(d) * (chunk // blk) + i
            yield n, pl.ds(pl.multiple_of(n * blk, blk), blk)

    @scoped("ret_states")
    def ret_states(d):
        for n, at in blocks_of(d):
            keys = rbuf[at, rkw : 2 * rkw].astype(F32) * hd ** (-0.5)
            for h in range(rheads):
                c = along[h, n]
                kd = (keys * jnp.exp(c[blk - 1 : blk, :1] - c[:, :1])).astype(BF16)
                values = rbuf[at, 2 * rkw + h * val : 2 * rkw + (h + 1) * val]
                upd[h, n] = jnp.where(ours(srow, h), tn(kd, values), 0.0)

    @scoped("ret_inner")
    def ret_inner(d):
        for n, at in blocks_of(d):
            keys = rbuf[at, rkw : 2 * rkw]
            for h in range(rheads):
                query = jnp.where(ours(rlane, h), rbuf[at, :rkw].astype(F32), 0.0)
                raw = nt(query.astype(BF16), keys)
                weights = (raw * hd ** (-0.5) * decay[h, n]).astype(BF16)
                rmid[h, at, :] = nn(weights, rbuf[at, 2 * rkw + h * val : 2 * rkw + (h + 1) * val])

    logrow = lax.broadcasted_iota(jnp.int32, (16, val), 0)

    def put_state(slot, state, logs):
        sts[slot, :rkw, :] = state.astype(BF16)
        tile = jnp.zeros((16, val), F32)
        for h in range(rheads):
            wide = jnp.broadcast_to(logs[h], (16, val))
            hi = wide.astype(BF16).astype(F32)
            tile = jnp.where(logrow == 2 * h, hi, tile)
            tile = jnp.where(logrow == 2 * h + 1, wide - hi, tile)
        sts[slot, rkw:, :] = tile.astype(BF16)

    def join(slot, states):
        piece = sts[slot, :rkw, :].astype(F32)
        logs = sts[slot, rkw:, :].astype(F32)
        return tuple(
            jnp.exp(logs[2 * h : 2 * h + 1] + logs[2 * h + 1 : 2 * h + 2]) * states[h]
            + jnp.where(ours(srow, h), piece, 0.0)
            for h in range(rheads)
        )

    def st_copy(k):
        return remote(sts.at[me], sts.at[me], st_send.at[k], st_recv.at[me],
                      {"sp": base + lax.rem(s + k, SQUARE)})

    def st_later(dg):
        return remote(sts.at[me], sts.at[me], st_up.at[dg], st_recv.at[me], {"sp": me + SQUARE * dg})

    def st_pass(back, k):
        span = me - SQUARE * (back + 1)
        return remote(sts.at[span], sts.at[span], st_on.at[back, k], st_recv.at[span],
                      {"sp": base + lax.rem(s + k, SQUARE)})

    def st_wait(span):
        remote(sts.at[span], sts.at[span], st_send.at[0], st_recv.at[span], pair).wait_recv()

    @scoped("span_state")
    def span_state():
        total = jnp.zeros((rkw, val), F32)
        logs = []
        for h in range(rheads):
            state = jnp.zeros((rkw, val), F32)
            log_all = jnp.zeros((1, 1), F32)
            for n in range(nblk):
                last = along[h, n, blk - 1 : blk, :1]
                state = jnp.exp(last) * state + upd[h, n]
                log_all = log_all + last
            total = total + state
            logs.append(log_all)
        put_state(me, total, logs)
        for k in range(1, SQUARE):

            @pl.when(s + k < SQUARE)
            def _():
                st_copy(k).start()

        for dg in range(1, ngroup):

            @pl.when(g + dg < ngroup)
            def _():
                st_later(dg).start()

    @scoped("pass_states")
    def pass_states():
        @pl.loop(0, g)
        def _(back):
            st_wait(me - SQUARE * (back + 1))
            for k in range(1, SQUARE):
                st_pass(back, k).start()

    @scoped("ret_finish")
    def ret_finish():
        first = []
        for h in range(rheads):
            parts = ([jnp.zeros((hd, val), F32)] * h + [init_ref[h]]
                     + [jnp.zeros((hd, val), F32)] * (rheads - 1 - h))
            first.append(jnp.concatenate(parts, axis=0) if rheads > 1 else parts[0])

        @pl.loop(0, g)
        def _(back):
            for k in range(1, SQUARE):
                st_wait(base - SQUARE * (back + 1) + lax.rem(s + k, SQUARE))

        @pl.loop(0, s)
        def _(slot):
            st_wait(base + slot)

        carried = lax.fori_loop(0, me, join, tuple(first))
        for h in range(rheads):
            state = carried[h]
            for n in range(nblk):
                at = slice(n * blk, (n + 1) * blk)
                c = along[h, n]
                query = rbuf[at, :rkw].astype(F32) * jnp.exp(c[:, :1])
                result = rmid[h, at, :] + nn(query, state, precision=HIGHEST)
                if n + 1 < nblk:
                    state = jnp.exp(c[blk - 1 : blk, :1]) * state + upd[h, n]
                mixr[at, h * val : (h + 1) * val] = head_norm(result).astype(BF16)

    decays()
    ret_states(0)
    ret_inner(0)
    to_later(0, steps(0)[0], 0)

    @scoped("take")
    def take(span, t, d, local):
        if local:
            here = (held[t] == s) & (head_core == core)

            @pl.when(here)
            def _():
                pltpu.make_async_copy(sndq.at[0, part(d)], qraw.at[t, part(d)], rq_sem.at[t, d]).wait()
                pltpu.make_async_copy(sndkv.at[0, part(d)], kvb.at[span, part(d)],
                                      rkv_sem.at[span, d]).wait()

            @pl.when(jnp.logical_not(here))
            def _():
                remote(qraw.at[t, part(d)], qraw.at[t, part(d)], sq_sem.at[0, d],
                       rq_sem.at[t, d], pair).wait_recv()
                remote(kvb.at[span, part(d)], kvb.at[span, part(d)], skv_sem.at[0, d],
                       rkv_sem.at[span, d], pair).wait_recv()
        else:
            remote(kvb.at[span, part(d)], kvb.at[span, part(d)], skv_sem.at[0, d],
                   rkv_sem.at[span, d], pair).wait_recv()

    def ready(t, d):
        tile = t * nchip + part(d)
        value = qraw[t, part(d)].astype(F32)
        qs[tile, :chunk] = jnp.where(lane < hd, value, 0.0).astype(BF16)
        qs[tile, chunk:] = jnp.where(lane < hd, 0.0, value).astype(BF16)

    def needs(t):
        return (core == 1) | (t == 0)

    def take_own(d):
        for t in range(2):
            take(base + held[t], t, d, True)

            @pl.when(needs(t))
            def _():
                fwd(base + held[t], t, 0, d).start()

        for t in range(2):
            ready(t, d)

    @scoped("take_own_pair")
    def take_own_pair(d):
        for t in range(2):

            @pl.when((core == 0) | (t == 0))
            def _():
                fwd(base + others[t], t, 0, d).wait_recv()

    krow = lax.broadcasted_iota(jnp.int32, (chunk, 2 * chunk), 0)
    qcol = lax.rem(lax.broadcasted_iota(jnp.int32, (chunk, 2 * chunk), 1), chunk)

    @scoped("attend")
    def attend(items, diagonal=False):
        scores = []
        for tile, blocks in items:
            row = []
            for span, a in blocks:
                keys = jnp.concatenate(
                    [kvb[span, a, 2 * c * own_rows : (2 * c + 1) * own_rows] for c in range(2)], axis=0)
                raw = nt(keys, qs[tile])
                row.append(jnp.where(krow <= qcol, raw, -jnp.inf) if diagonal else raw)
            scores.append(row)
        for (tile, blocks), row in zip(items, scores):
            old = peak[tile]
            top = old
            for raw in row:
                top = jnp.maximum(top, jnp.max(raw, axis=0, keepdims=True))
            rescale = jnp.exp(old - top)
            total = None
            weighted = None
            for (span, a), raw in zip(blocks, row):
                e = jnp.exp(raw - top[:1])
                sums = jnp.sum(e.reshape(chunk // 8, 8, 2 * chunk), axis=0)
                turned = jnp.concatenate(
                    [kvb[span, a, (2 * c + 1) * own_rows : (2 * c + 2) * own_rows] for c in range(2)],
                    axis=1)
                got = nn(turned, e.astype(BF16))
                total = sums if total is None else total + sums
                weighted = got if weighted is None else weighted + got
            peak[tile] = top
            den[tile] = den[tile] * rescale + total
            acc[tile] = acc[tile] * rescale[:1] + weighted

    def tile_of(t, d):
        return t * nchip + part(d)

    def prior_keys(queries_d, keys_d, fresh):
        @pl.loop(0, g)
        def _(back):
            first = SQUARE * (g - 1 - back)
            for group in range(2):
                slots = held if group == 0 else others
                spans = [first + slots[t] for t in range(2)]
                if fresh:
                    for t in range(2):
                        if group == 0:
                            take(spans[t], t, keys_d, False)
                            fwd(spans[t], t, 1 + back, keys_d).start()
                        else:
                            take(spans[t], t, keys_d, False)
                for e in queries_d:
                    attend([(tile_of(t, e), [(span, part(keys_d)) for span in spans]) for t in range(2)])

    def own_whole(queries_d, keys_d):
        third_t, third_slot = 1 - core, 2 * (1 - core)
        at = part(keys_d)
        attend([item for e in queries_d for item in (
            (nchip + part(e), ((base, at), (base + 1, at))),
            (third_t * nchip + part(e), ((base + third_slot, at),)),
        )])

    width = out_ref.shape[1]
    cut = mine.shape[2]
    npiece = width // cut

    def mixed_rows(which):
        return mixr[pl.ds(pl.multiple_of(which * chunk, chunk), chunk), :]

    def split(d, n, full):
        first, second = full[:own_rows], full[own_rows:]
        mine[d * npiece + n] = jnp.where(core == 0, second, first).astype(BF16)
        kept[d * npiece + n] = jnp.where(core == 0, first, second)
        pair_copy(d, n).start()

    def pair_copy(d, n):
        return remote(mine.at[d * npiece + n], from_pair.at[d * npiece + n], mpair_send.at[d, n],
                      mpair_recv.at[d, n], pair)

    def chip_copy(d, n):
        there = lax.rem(chip + d, nchip) * 2 + core
        return remote(sent.at[d * npiece + n], from_chip.at[d * npiece + n], mchip_send.at[d, n],
                      mchip_recv.at[d, n], {"tp": there})

    @scoped("ret_reduce")
    def ret_reduce():
        out_loads[1].wait()
        for d in range(1, nchip):
            which = lax.rem(chip + d, nchip)
            for n in range(npiece):
                split(d, n, nn(mixed_rows(which), wobuf[depth:, n * cut : (n + 1) * cut]))

    @scoped("ret_send")
    def ret_send():
        for d in range(1, nchip):
            for n in range(npiece):
                pair_copy(d, n).wait_recv()
                at = d * npiece + n
                sent[at] = (kept[at] + from_pair[at].astype(F32)).astype(BF16)
                if n < npiece - 1:
                    chip_copy(d, n).start()

    def slab_in(d, which):
        index = part(d) * 2 + which
        for half in range(2):
            landed(index, half)

            @pl.when(core == which)
            def _():
                pair_slab(index, half).start()

    for d in range(1, nchip):
        slab_in(d, 0)
        project(d, steps(d)[0])

    for d in range(1, nchip):
        slab_in(d, 1)
        if d == nchip - 1:
            out_loads[0].wait()
            for e in range(1, nchip):
                for n in range(2):
                    w_cross(e, n).start()
        project_ret(d)
        ret_states(d)
        if d == nchip - 1:
            span_state()
        project(d, steps(d)[1])
        if d < nchip - 1:
            for step in steps(d):
                to_later(d, step, 1)
        ret_inner(d)
    take_own(0)
    attend([(tile_of(t, 0), [(base + held[t], part(0))]) for t in range(2)], diagonal=True)
    take_own_pair(0)
    own_whole([0], 0)
    pass_states()
    for d in range(1, nchip):
        for step in steps(d):
            to_later(d, step, 0)
    prior_keys([0], 0, True)

    lam_copy(1 - core).wait_recv()
    lam = lamv[head_core, pl.ds(pl.multiple_of(8 * head_no, 8), 8), :][:1, :1]

    def d_copy(t, d):
        where = {"sp": base + held[t], "tp": part(d) * 2 + head_core}
        return remote(dsend.at[t, part(d)], dret.at[chip, head_no], ds_sem.at[t, d],
                      rd_sem.at[chip, head_no], where)

    def d_local(t, d):
        return pltpu.make_async_copy(dsend.at[t, part(d)], dret.at[chip, head_no],
                                     rd_sem.at[chip, head_no])

    def home(t, d):
        return (held[t] == s) & (head_core == core) if d == 0 else False

    @scoped("finish")
    def finish(t, d):
        tile = tile_of(t, d)
        scale = 1.0 / jnp.sum(den[tile], axis=0, keepdims=True)
        out = acc[tile] * scale
        merged = out[:, :chunk] - lam * out[:, chunk:]
        square = jnp.mean(merged * merged, axis=0, keepdims=True)
        normed = (merged * lax.rsqrt(square + HEAD_EPS)).T
        dsend[t, part(d)] = (normed * gain_ref[...] * DIFF_SCALE).astype(BF16)
        if d:
            d_copy(t, d).start()
        else:

            @pl.when(home(t, d))
            def _():
                d_local(t, d).start()

            @pl.when(jnp.logical_not(home(t, d)))
            def _():
                d_copy(t, d).start()

    for d in range(1, nchip):
        take_own(d)
        if d == nchip - 1:
            w_pass(0)
            ret_finish()
            ret_reduce()
            w_pass(1)
        for e in range(d):
            own_whole([d], e)
            if d == nchip - 1 and e == 0:
                ret_send()
                for step in steps(d):
                    to_later(d, step, 1)
            prior_keys([d], e, False)
            high = jnp.maximum(part(d), part(e))
            low = jnp.minimum(part(d), part(e))
            attend([(t * nchip + high, [(base + held[t], low)]) for t in range(2)])
        attend([(tile_of(t, d), [(base + held[t], part(d))]) for t in range(2)], diagonal=True)
        take_own_pair(d)
        own_whole(list(range(d + 1)), d)
        if d < nchip - 1:
            prior_keys(list(range(d + 1)), d, True)

    last = nchip - 1
    prior_keys(list(range(1, nchip)), last, True)
    for d in range(1, nchip):
        for t in range(2):
            finish(t, d)
    for d in range(1, nchip):
        chip_copy(d, npiece - 1).start()
    prior_keys([0], last, False)
    for t in range(2):
        finish(t, 0)


    for d in range(1, nchip):
        for n in range(2):
            with jax.named_scope("w_last"):
                w_side(d, 1 - b, n).wait_recv()
    for h in range(heads):
        for d in range(nchip):
            source = lax.rem(chip + d, nchip)
            piece = dret.at[source, h]
            arrival = remote(piece, piece, ds_sem.at[0, d], rd_sem.at[source, h], pair)
            if d:
                with jax.named_scope("d_wait"):
                    arrival.wait_recv()
            else:

                @pl.when(stays(h))
                def _():
                    pltpu.make_async_copy(dsend.at[0, chip], piece, rd_sem.at[source, h]).wait()

                @pl.when(jnp.logical_not(stays(h)))
                def _():
                    with jax.named_scope("d_wait"):
                        arrival.wait_recv()

    def partial(n):
        total = nn(
            jnp.concatenate([dret[chip, h] for h in range(heads)] + [mixed_rows(chip)], axis=1),
            wobuf[:, n * cut : (n + 1) * cut])
        for d in range(1, nchip):
            source = lax.rem(chip + d, nchip)
            total = total + nn(
                jnp.concatenate([dret[source, h] for h in range(heads)], axis=1),
                wx[d - 1, :, n * cut : (n + 1) * cut])
        return total

    def put(n):
        return pltpu.make_async_copy(outv.at[n], out_ref.at[:, n * cut : (n + 1) * cut], osem.at[n])

    for n in range(npiece):
        split(0, n, partial(n))
    for n in range(npiece):
        with jax.named_scope("p_wait"):
            pair_copy(0, n).wait_recv()
        total = kept[n] + from_pair[n].astype(F32)
        for d in range(1, nchip):
            with jax.named_scope("c_wait"):
                chip_copy(d, n).wait_recv()
            total = total + from_chip[d * npiece + n].astype(F32)
        outv[n] = total.astype(BF16)
        put(n).start()

    with jax.named_scope("s_wait"):
        for copy in copies:
            copy.wait_send()

    for d in range(nchip):
        for h in range(heads):

            @pl.when(jnp.logical_not(stays(h)))
            def _():
                for step in steps(d):
                    q_copy(h, d, step).wait_send()
                    kv_copy(h, d, 0, step).wait_send()

        for dg in range(1, ngroup):

            @pl.when(g + dg < ngroup)
            def _():
                for h in range(heads):
                    for step in steps(d):
                        kv_copy(h, d, dg, step).wait_send()

        for t in range(2):

            @pl.when(needs(t))
            def _():
                fwd(base + held[t], t, 0, d).wait_send()

            if d:
                d_copy(t, d).wait_send()
            else:

                @pl.when(jnp.logical_not(home(t, d)))
                def _():
                    d_copy(t, d).wait_send()

        @pl.loop(0, g)
        def _(back):
            for t in range(2):
                fwd(SQUARE * (g - 1 - back) + held[t], t, 1 + back, d).wait_send()

    for d in range(1, nchip):
        for n in range(2):
            w_cross(d, n).wait_send()
            w_side(d, b, n).wait_send()
    for k in range(1, SQUARE):

        @pl.when(s + k < SQUARE)
        def _():
            st_copy(k).wait_send()

        @pl.loop(0, g)
        def _(back):
            st_pass(back, k).wait_send()

    for dg in range(1, ngroup):

        @pl.when(g + dg < ngroup)
        def _():
            st_later(dg).wait_send()

    for d in range(nchip):
        for n in range(npiece):
            pair_copy(d, n).wait_send()
            if d:
                chip_copy(d, n).wait_send()
    for n in range(npiece):
        put(n).wait()


VMEM = pl.BlockSpec(memory_space=pltpu.VMEM)
ANY = pl.BlockSpec(memory_space=pl.ANY)
SMEM = pl.BlockSpec(memory_space=pltpu.SMEM)
DMA = pltpu.SemaphoreType.DMA


def params(number):
    return pltpu.CompilerParams(
        collective_id=number, has_side_effects=True, vmem_limit_bytes=VMEM_LIMIT,
    )


def on_device(nsp, ntp, tokens, norm_gain, w_query_one, w_query_two, w_key_one, w_key_two, w_value,
              mix_lambda, head_gain, w_ret_query, w_ret_key, w_ret_value, retain_log, init_state,
              w_out_diff, w_out_ret):
    weights = (w_query_one, w_query_two, w_key_one, w_key_two, w_value, w_ret_query, w_ret_key, w_ret_value)
    widths = tuple(w.shape[1] for w in weights)
    own_rows, model = tokens.shape
    rows = own_rows * ntp
    nchip = ntp // 2
    ngroup = nsp // SQUARE
    chunk = rows // nchip
    heads = mix_lambda.shape[0]
    rheads, hd, val = init_state.shape
    kw = widths[2]
    width = w_out_diff.shape[1]
    npiece = 4
    cut = width // npiece
    return pl.pallas_call(
        functools.partial(layer_kernel, nsp, ntp, widths, heads, rheads),
        out_shape=jax.ShapeDtypeStruct((own_rows, width), BF16),
        in_specs=[SMEM] + [VMEM] * 5 + [ANY] * (len(weights) + 2),
        out_specs=ANY,
        scratch_shapes=[
            pltpu.VMEM((ntp, own_rows, model), BF16),
            pltpu.VMEM((model, sum(widths)), BF16),
            pltpu.VMEM((w_out_diff.shape[0] + w_out_ret.shape[0], width), BF16),
            pltpu.VMEM((nchip - 1, w_out_diff.shape[0], width), BF16),
            pltpu.VMEM((heads, nchip, chunk, kw), BF16),
            pltpu.VMEM((heads, nchip, 2 * chunk, kw), BF16),
            pltpu.VMEM((nsp, nchip, 2 * chunk, kw), BF16),
            pltpu.VMEM((2, nchip, chunk, kw), BF16),
            pltpu.VMEM((2 * nchip, 2 * chunk, kw), BF16),
            pltpu.VMEM((2, 8 * heads, 128), F32),
            pltpu.VMEM((2 * nchip, 8, 2 * chunk), F32),
            pltpu.VMEM((2 * nchip, 8, 2 * chunk), F32),
            pltpu.VMEM((2 * nchip, val, 2 * chunk), F32),
            pltpu.VMEM((2, nchip, chunk, val), BF16),
            pltpu.VMEM((nchip, heads, chunk, val), BF16),
            pltpu.VMEM((nsp, rheads * hd + 16, val), BF16),
            pltpu.VMEM((rows, sum(widths[5:])), BF16),
            pltpu.VMEM((rheads, rows // BLOCK, BLOCK, BLOCK), F32),
            pltpu.VMEM((rheads, rows // BLOCK, BLOCK, 128), F32),
            pltpu.VMEM((rheads, rows, val), F32),
            pltpu.VMEM((rheads, rows // BLOCK, rheads * hd, val), F32),
            pltpu.VMEM((rows, rheads * val), BF16),
            pltpu.VMEM((nchip * npiece, own_rows, cut), BF16),
            pltpu.VMEM((nchip * npiece, own_rows, cut), BF16),
            pltpu.VMEM((nchip * npiece, own_rows, cut), BF16),
            pltpu.VMEM((nchip * npiece, own_rows, cut), BF16),
            pltpu.VMEM((nchip * npiece, own_rows, cut), F32),
            pltpu.VMEM((npiece, own_rows, cut), BF16),
            DMA((len(weights) + 2,)),
            DMA((2,)),
            DMA((nchip, 2)),
            DMA((nchip, 2)),
            DMA((ntp, 2)),
            DMA((nchip - 1, 2)),
            DMA((nchip - 1, 2)),
            DMA((nchip - 1, 2, 2)),
            DMA((heads, 2 * nchip - 1)),
            DMA((heads, 2 * nchip - 1)),
            DMA((max(ngroup - 1, 1), heads, 2 * nchip - 1)),
            DMA((ngroup, 2, nchip)),
            DMA((2, nchip)),
            DMA((nsp, nchip)),
            DMA((2, nchip)),
            DMA((nchip, heads)),
            DMA((SQUARE,)),
            DMA((ngroup,)),
            DMA((ngroup, SQUARE)),
            DMA((nsp,)),
            DMA((nchip, npiece)),
            DMA((nchip, npiece)),
            DMA((nchip, npiece)),
            DMA((nchip, npiece)),
            DMA((npiece,)),
        ],
        compiler_params=params(0),
        name="layer",
    )(mix_lambda, tokens, norm_gain[None, :], head_gain[None, :], retain_log, init_state, *weights,
      w_out_diff, w_out_ret)


def solution(mesh):
    in_specs = (
        P(("sp", "tp"), None),
        P(),
        P(None, "tp"),
        P(None, "tp"),
        P(None, "tp"),
        P(None, "tp"),
        P(None, "tp"),
        P("tp"),
        P(),
        P(None, "tp"),
        P(None, "tp"),
        P(None, "tp"),
        P("tp", "sp"),
        P("tp", None, None),
        P("tp", None),
        P("tp", None),
    )
    body = functools.partial(on_device, mesh.shape["sp"], mesh.shape["tp"])
    return jax.shard_map(
        body, mesh=mesh, in_specs=in_specs, out_specs=P(("sp", "tp"), None), check_vma=False
    )
```
